512 devices in a mesh: fs: 16 (over y, x), tp: 32 (over z, core).
Axes of the slice: x: 4, y: 4, z: 16, core: 2. Of those that a mesh axis runs over, the one named last changes fastest.
Arguments:
- saved_input: bfloat16 [16384, 4096], P('fs', 'tp'), may hold values from -6 to 6
- query_cot: bfloat16 [16384, 4096], P('fs', 'tp'), may hold values from -6 to 6
- key_cot: bfloat16 [16384, 4096], P('fs', 'tp'), may hold values from -6 to 6
- query_master: float32 [4096, 4096], P('fs', 'tp'), may hold values from -0.09375 to 0.09375
- key_master: float32 [4096, 4096], P('fs', 'tp'), may hold values from -0.09375 to 0.09375
- query_basis: bfloat16 [4096, 256], P('fs'), may hold values from -3 to 3
- key_basis: bfloat16 [4096, 256], P('fs'), may hold values from -3 to 3
- query_first: float32 [256, 4096], P('fs', 'tp'), may hold values from -240 to 240
- query_second: float32 [256, 4096], P('fs', 'tp'), may hold values from 1000 to 20000
- key_first: float32 [256, 4096], P('fs', 'tp'), may hold values from -240 to 240
- key_second: float32 [256, 4096], P('fs', 'tp'), may hold values from 1000 to 20000
Outputs:
- query_step: float32 [4096, 4096], P('fs', 'tp')
- query_weight: float32 [4096, 4096], P('fs', 'tp')
- query_copy: bfloat16 [4096, 4096], P(None, 'tp')
- query_first_new: float32 [256, 4096], P('fs', 'tp')
- query_second_new: float32 [256, 4096], P('fs', 'tp')
- key_step: float32 [4096, 4096], P('fs', 'tp')
- key_weight: float32 [4096, 4096], P('fs', 'tp')
- key_copy: bfloat16 [4096, 4096], P(None, 'tp')
- key_first_new: float32 [256, 4096], P('fs', 'tp')
- key_second_new: float32 [256, 4096], P('fs', 'tp')
The draws below stay inside these ranges and needn't reach their ends.
All inputs are finite; a program needn't handle non-finite values.
Results may differ from the reference program's by a relative error of at most 0.0065.
Values may be sent and summed in bfloat16 or wider, within the bound.
A program may use at most 64 MiB of HBM per device.

```python
import math
import jax
import jax.numpy as jnp
from jax import lax

D = 4096
HEADS = 32
HD = 128
RANK = 256
TOKENS = 16384


def basis_draw(key, salt):
    base = jax.random.fold_in(key, salt)
    entry_key, factor_key = jax.random.split(base)
    group = max(D // 64, 1)
    groups = D // group
    entries = jnp.clip(jax.random.normal(entry_key, (D, RANK), jnp.float32), -4.0, 4.0)
    factors = jnp.exp(jax.random.uniform(factor_key, (groups,), jnp.float32, -1.5, 1.5))
    row_scale = jnp.repeat(factors, group)
    values = entries * row_scale[:, None] * D ** (-0.5)
    return values.astype(jnp.bfloat16)


def draw_query_basis(key, part):
    return basis_draw(key, 101)


def draw_key_basis(key, part):
    return basis_draw(key, 202)


def block_scale(key, dims, pieces, low, largest):
    loudness, own = 1.0, jax.random.fold_in(key, 6)
    for position, blocks in pieces:
        steps = jnp.exp(jax.random.uniform(jax.random.fold_in(own, position), (blocks,), jnp.float32, low / len(pieces), largest / len(pieces)))
        loudness = loudness * jnp.repeat(steps, dims[position] // blocks).reshape([-1 if axis == position else 1 for axis in range(len(dims))])
    return loudness


def bell_draw(stream_key, shape, scale, most, cuts=(), kind=jnp.bfloat16):
    values = jax.random.normal(stream_key, shape, jnp.float32) * scale
    if len(cuts) > 0:
        values = block_scale(stream_key, shape, cuts, -0.22, 0.18) * values
    return jnp.clip(values, min=-most, max=most).astype(kind)


def setup_inputs(seed: int = 0) -> dict:
    seeds = jax.random.split(jax.random.key(seed), 12)
    saved_input = bell_draw(seeds[0], (TOKENS, D), 1.0, 6.0, ((0, 16), (1, 32)))
    query_cot = bell_draw(seeds[1], (TOKENS, HEADS * HD), 1.0, 6.0, ((0, 16), (1, 32)))
    key_cot = bell_draw(seeds[2], (TOKENS, HEADS * HD), 1.0, 6.0, ((0, 16), (1, 32)))
    query_master = bell_draw(seeds[3], (D, HEADS * HD), D ** -0.5, 0.09375, ((0, 16), (1, 32)), jnp.float32)
    key_master = bell_draw(seeds[4], (D, HEADS * HD), D ** -0.5, 0.09375, ((0, 16), (1, 32)), jnp.float32)
    query_basis = draw_query_basis(jax.random.fold_in(seeds[11], 71), 0)
    key_basis = draw_key_basis(jax.random.fold_in(seeds[11], 71), 0)
    query_first = bell_draw(seeds[7], (RANK, HEADS * HD), 40.0, 240.0, ((0, 16), (1, 32)), jnp.float32)
    query_second = jnp.clip(jnp.exp(math.log(20000.0) - 2.9957323 * jax.random.uniform(seeds[8], (RANK, HEADS * HD), jnp.float32) ** block_scale(seeds[8], (RANK, HEADS * HD), ((0, 16), (1, 32)), -0.2, 0.2)), 1000.0, 20000.0)
    key_first = bell_draw(seeds[9], (RANK, HEADS * HD), 40.0, 240.0, ((0, 16), (1, 32)), jnp.float32)
    key_second = jnp.clip(jnp.exp(math.log(20000.0) - 2.9957323 * jax.random.uniform(seeds[10], (RANK, HEADS * HD), jnp.float32) ** block_scale(seeds[10], (RANK, HEADS * HD), ((0, 16), (1, 32)), -0.2, 0.2)), 1000.0, 20000.0)
    return {"saved_input": saved_input, "query_cot": query_cot, "key_cot": key_cot, "query_master": query_master, "key_master": key_master, "query_basis": query_basis, "key_basis": key_basis, "query_first": query_first, "query_second": query_second, "key_first": key_first, "key_second": key_second}


moment_decay = 0.8
square_decay = 0.9
square_floor = 1.0
norm_floor = 0.01
step_rate = 0.01

def update_one(saved_input, cotangent, master, basis, first, second):
    grad = jnp.dot(saved_input.T, cotangent, preferred_element_type=jnp.float32)
    low = jnp.dot(basis.astype(jnp.float32).T, grad, precision=lax.Precision.HIGHEST)
    first_new = moment_decay * first + (1.0 - moment_decay) * low
    second_new = square_decay * second + (1.0 - square_decay) * low * low
    ratio = (first_new / jnp.sqrt(second_new + square_floor)).astype(jnp.bfloat16)
    update = jnp.dot(basis, ratio, preferred_element_type=jnp.float32)
    by_head = update.reshape(D, HEADS, HD)
    head_mean = lax.optimization_barrier(jnp.mean(by_head * by_head, axis=(0, 2)))
    head_scale = 1.0 / jnp.sqrt(head_mean + norm_floor)
    step = (by_head * head_scale[None, :, None]).reshape(D, HEADS * HD)
    weight = master - step_rate * step
    return (step, weight, weight.astype(jnp.bfloat16), first_new, second_new)

def reference(saved_input, query_cot, key_cot, query_master, key_master, query_basis, key_basis, query_first, query_second, key_first, key_second):
    query_out = update_one(saved_input, query_cot, query_master, query_basis, query_first, query_second)
    key_out = update_one(saved_input, key_cot, key_master, key_basis, key_first, key_second)
    return (query_out[0], query_out[1], query_out[2], query_out[3], query_out[4], key_out[0], key_out[1], key_out[2], key_out[3], key_out[4])
```

```python
import jax
import jax.numpy as jnp
from jax import lax
from jax.experimental import pallas as pl
from jax.experimental.pallas import tpu as pltpu
from jax.sharding import Mesh
from jax.sharding import PartitionSpec as P

D = 4096
HD = 128
RANK = 256
YN, XN, ZN, CN = 4, 4, 16, 2
FN = YN * XN
TOK = 1024
SUB = TOK // ZN
ROWS = D // FN
HALF = ROWS // CN
LOW = RANK // FN
AXES = ("y", "x", "z", "c")
FS = ("y", "x")
TP = ("z", "c")

moment_decay = 0.8
square_decay = 0.9
square_floor = 1.0
norm_floor = 0.01
step_rate = 0.01

MESH_ID = pl.DeviceIdType.MESH
BF = jnp.bfloat16
F32 = jnp.float32

PLANE = sorted(
    [(dy, dx) for dy in range(YN) for dx in range(XN) if (dy, dx) != (0, 0)],
    key=lambda o: -(min(o[0], 4 - o[0]) + min(o[1], 4 - o[1])),
)
ALONG_Z = [8, 7, -7, 6, -6, 5, -5, 4, -4, 3, -3, 2, -2, 1, -1]
Z_FIRST = [6, -6, 3, -3, 1, -1]
Z_RELAY = [(3, (1, -1)), (-3, (-1, 1)), (6, (2, 1, -1)), (-6, (-1, 1))]


class Sends:
    def __init__(self, send_sem, recv_sem):
        self.send_sem, self.recv_sem = send_sem, recv_sem
        self.count = 0
        self.started = []

    def take(self):
        self.count += 1
        return self.count - 1

    def start(self, number, src, dst, device):
        copy = pltpu.make_async_remote_copy(
            src_ref=src,
            dst_ref=dst,
            send_sem=self.send_sem.at[number],
            recv_sem=self.recv_sem.at[number],
            device_id=device,
            device_id_type=MESH_ID,
        )
        copy.start()
        self.started.append(copy)

    def landed(self, number, dst, device):
        pltpu.make_async_remote_copy(
            src_ref=dst,
            dst_ref=dst,
            send_sem=self.send_sem.at[number],
            recv_sem=self.recv_sem.at[number],
            device_id=device,
            device_id_type=MESH_ID,
        ).wait_recv()

    def finish(self):
        for copy in self.started:
            copy.wait_send()


def wrap(value, count):
    return lax.rem(value + 2 * count, count)


def plane_gather(sends, piece, me, rows):
    y, x, z, c = me
    half, quarter = rows // 2, rows // 4
    signs = (1, -1)

    def shift(h, first, second):
        d1, d2 = (first, second)
        dy, dx = (d2, d1) if h == 0 else (d1, d2)
        return wrap(y + dy, YN), wrap(x + dx, XN)

    def ref(h, first, second, part=None):
        fy, fx = shift(h, first, second)
        start = h * half + (0 if part is None else part * quarter)
        return piece(fy, fx, start, half if part is None else quarter)

    def dev(h, first, second):
        fy, fx = shift(h, first, second)
        return (fy, fx, z, c)

    part_of = {1: 0, -1: 1}
    both = [(h, s) for h in (0, 1) for s in signs]
    n1 = {k: sends.take() for k in both}
    n1r = {k: sends.take() for k in both}
    n2 = {(h, j, s): sends.take() for j in (0, -1, 1, 2) for h, s in both}
    n2r = {(h, j, s): sends.take() for j in (0, -1, 1, 2) for h, s in both}

    def second_stage(h, j):
        for s in signs:
            sends.start(n2[h, j, s], ref(h, j, 0), ref(h, j, 0), dev(h, 0, s))

    def second_relay(h, j):
        for s in signs:
            sends.landed(n2[h, j, s], ref(h, j, -s), dev(h, 0, s))
            p = part_of[s]
            sends.start(n2r[h, j, s], ref(h, j, -s, p), ref(h, j, -s, p), dev(h, 0, s))

    for h, s in both:
        sends.start(n1[h, s], ref(h, 0, 0), ref(h, 0, 0), dev(h, s, 0))
    for h in (0, 1):
        second_stage(h, 0)
    yield
    for h, s in both:
        sends.landed(n1[h, s], ref(h, -s, 0), dev(h, s, 0))
        p = part_of[s]
        sends.start(n1r[h, s], ref(h, -s, 0, p), ref(h, -s, 0, p), dev(h, s, 0))
        second_stage(h, -s)
    yield
    for h in (0, 1):
        second_relay(h, 0)
    yield
    for h in (0, 1):
        for s in signs:
            p = part_of[s]
            sends.landed(n1r[h, s], ref(h, 2, 0, p), dev(h, s, 0))
        second_stage(h, 2)
    yield
    for j in (-1, 1):
        for h in (0, 1):
            second_relay(h, j)
    yield
    for h in (0, 1):
        second_relay(h, 2)
    yield
    for j in (0, -1, 1, 2):
        for h, s in both:
            p = part_of[s]
            sends.landed(n2r[h, j, s], ref(h, j, 2, p), dev(h, s, 0))


def exchange(
    x_in, qc_in, kc_in, qm_in, km_in, qb_in, kb_in, qf_in, qs_in, kf_in, ks_in,
    basis, masters, ratios, moments_out,
    xs, xg, cots, cot_other, cot_rel, cot_t, mas, mom, mom_other,
    psend, precv, xb, lowp, lowr, rsend, msend,
    load_sem, send_sem, recv_sem,
):
    y, x, z, c = (lax.axis_index(a) for a in AXES)
    me = (y, x, z, c)
    oc = 1 - c
    f = y * XN + x
    partner = (y, x, z, oc)

    barrier = pltpu.get_barrier_semaphore()
    near = [(wrap(y + dy, YN), wrap(x + dx, XN), z, c) for dy, dx in PLANE]
    near += [(wrap(y + dy, YN), wrap(x + dx, XN), z, oc) for dy, dx in PLANE]
    near += [partner]
    near += [(y, x, wrap(z + d, ZN), c) for d in ALONG_Z]
    for device in near:
        pl.semaphore_signal(barrier, inc=1, device_id=device, device_id_type=MESH_ID)

    loads = []

    def load(src, dst):
        copy = pltpu.make_async_copy(src, dst, load_sem.at[len(loads)])
        copy.start()
        loads.append(copy)

    mine = pl.ds(pl.multiple_of(c * HALF, HALF), HALF)
    load(x_in, xs)
    load(qb_in.at[mine], basis.at[f, c, :, pl.ds(0, RANK)])
    load(kb_in.at[mine], basis.at[f, c, :, pl.ds(RANK, RANK)])
    load(qc_in, cots.at[0])
    load(kc_in, cots.at[1])
    load(qf_in, mom.at[0, 0])
    load(qs_in, mom.at[0, 1])
    load(kf_in, mom.at[1, 0])
    load(ks_in, mom.at[1, 1])
    load(qm_in, mas.at[0])
    load(km_in, mas.at[1])
    for copy in loads:
        copy.wait()
    masters[f, :, 0:HD] = mas[0].astype(BF)
    masters[f, :, HD : 2 * HD] = mas[1].astype(BF)

    sends = Sends(send_sem, recv_sem)
    pl.semaphore_wait(barrier, len(near))

    def xslot(zz):
        return xg.at[:, pl.ds(pl.multiple_of(zz * HD, HD), HD)]

    nx = {d: sends.take() for d in ALONG_Z}
    gather_basis = plane_gather(
        sends, lambda fy, fx, s, n: basis.at[fy * XN + fx, c, pl.ds(s, n)], me, HALF
    )
    gather_masters = plane_gather(
        sends, lambda fy, fx, s, n: masters.at[fy * XN + fx, pl.ds(s, n)], me, ROWS
    )
    next(gather_basis)
    for d in ALONG_Z:
        zz = wrap(z + d, ZN)
        rows = xs.at[pl.ds(pl.multiple_of(zz * SUB, SUB), SUB)]
        sends.start(nx[d], rows, xslot(z), (y, x, zz, c))
    n_cot, n_mom = sends.take(), sends.take()
    sends.start(n_cot, cots.at[oc], cot_other, partner)
    sends.start(n_mom, mom.at[oc], mom_other, partner)
    xg[:, pl.ds(pl.multiple_of(z * HD, HD), HD)] = xs[pl.ds(pl.multiple_of(z * SUB, SUB), SUB), :]
    next(gather_basis)

    sends.landed(n_cot, cot_other, partner)
    sends.landed(n_mom, mom_other, partner)
    for o in range(ZN):
        zz = wrap(z - o, ZN)
        rows = pl.ds(pl.multiple_of(zz * SUB, SUB), SUB)
        cot_rel[o * SUB : (o + 1) * SUB, 0:HD] = cots[c, rows, :]
        cot_rel[o * SUB : (o + 1) * SUB, HD : 2 * HD] = cot_other[rows, :]
    next(gather_basis)
    next(gather_basis)
    cot_t[...] = cot_rel[...].T
    for _ in gather_basis:
        pass
    next(gather_masters)
    for d in ALONG_Z:
        sends.landed(nx[d], xslot(wrap(z - d, ZN)), partner)

    part = jnp.zeros((SUB, 2 * RANK), F32)
    for k in range(FN // 2):
        rows = basis[2 * k : 2 * k + 2, c].reshape(2 * HALF, 2 * RANK)
        part += jnp.dot(
            xg[:, k * 2 * HD : (k + 1) * 2 * HD], rows, preferred_element_type=F32
        )
    psend[0] = part[:, :RANK]
    psend[1] = part[:, RANK:]
    n_part = sends.take()
    sends.start(n_part, psend.at[oc], precv, partner)
    n_basis = sends.take()
    sends.landed(n_part, precv, partner)
    xb[0] = (psend[c] + precv[...]).astype(BF)

    nz = {}
    for d in Z_FIRST:
        nz[d % ZN] = sends.take()
    for o, hops in Z_RELAY:
        for d in hops:
            nz[(o + d) % ZN] = sends.take()
    seen = set()

    def z_send(o, d):
        sends.start(
            nz[(o + d) % ZN], xb.at[o % ZN], xb.at[(o + d) % ZN], (y, x, wrap(z + d, ZN), c)
        )

    def z_landed(o):
        if o % ZN not in seen:
            seen.add(o % ZN)
            sends.landed(nz[o % ZN], xb.at[o % ZN], partner)

    for d in Z_FIRST:
        z_send(0, d)
    sends.start(n_basis, basis.at[:, c], basis.at[:, c], partner)
    next(gather_masters)
    for o, hops in Z_RELAY[:2]:
        z_landed(o)
        for d in hops:
            z_send(o, d)
    for o, hops in Z_RELAY[2:]:
        z_landed(o)
        for d in hops:
            z_send(o, d)
    next(gather_masters)
    next(gather_masters)
    next(gather_masters)
    for o in range(1, ZN):
        z_landed(o)

    low_t = jnp.dot(cot_t[...], xb[...].reshape(TOK, RANK), preferred_element_type=F32)
    lowp[...] = low_t.T.reshape(FN, LOW, 2 * HD)
    nl = {p: sends.take() for p in PLANE}
    for dy, dx in PLANE:
        ty, tx = wrap(y + dy, YN), wrap(x + dx, XN)
        sends.start(nl[dy, dx], lowp.at[ty * XN + tx], lowr.at[dy * XN + dx], (ty, tx, z, c))
    next(gather_masters)
    low = lowp[f]
    for dy, dx in PLANE:
        sends.landed(nl[dy, dx], lowr.at[dy * XN + dx], partner)
        low = low + lowr[dy * XN + dx]

    nr = {(p, k): sends.take() for p in [(0, 0)] + PLANE for k in (0, 1)}
    n_out = sends.take()
    for k, (first, second) in enumerate(
        ((mom[c, 0], mom[c, 1]), (mom_other[0], mom_other[1]))
    ):
        part = low[:, k * HD : (k + 1) * HD]
        first_new = moment_decay * first + (1.0 - moment_decay) * part
        second_new = square_decay * second + (1.0 - square_decay) * part * part
        rsend[k] = (first_new / jnp.sqrt(second_new + square_floor)).astype(BF)
        if k == 0:
            moments_out[c, 0] = first_new
            moments_out[c, 1] = second_new
        else:
            msend[0] = first_new
            msend[1] = second_new
    ratios[c, f] = rsend[0]
    for dy, dx in PLANE + [(0, 0)]:
        ty, tx = wrap(y + dy, YN), wrap(x + dx, XN)
        for k, core in ((0, c), (1, oc)):
            if k == 0 and (dy, dx) == (0, 0):
                continue
            sends.start(nr[(dy, dx), k], rsend.at[k], ratios.at[c, f], (ty, tx, z, core))
    sends.start(n_out, msend, moments_out.at[c], partner)
    for _ in gather_masters:
        pass
    sends.landed(n_basis, basis.at[:, oc], partner)
    for dy, dx in PLANE + [(0, 0)]:
        sy, sx = wrap(y - dy, YN), wrap(x - dx, XN)
        for k in (0, 1):
            if k == 0 and (dy, dx) == (0, 0):
                continue
            m = c if k == 0 else oc
            sends.landed(nr[(dy, dx), k], ratios.at[m, sy * XN + sx], partner)
    sends.landed(n_out, moments_out.at[oc], partner)
    sends.finish()


N_SENDS = 15 + 80 + 2 + 2 + 15 + 15 + 32 + 1


def finish(
    basis, masters, ratios, moments, qm, km,
    q_step, q_weight, q_copy, q_first, q_second,
    k_step, k_weight, k_copy, k_first, k_second,
    held,
):
    f = lax.axis_index("y") * XN + lax.axis_index("x")
    outs = (
        (qm, q_step, q_weight, q_copy, q_first, q_second),
        (km, k_step, k_weight, k_copy, k_first, k_second),
    )
    for m, (master, step_ref, weight_ref, copy_ref, first_ref, second_ref) in enumerate(outs):
        first_ref[...] = moments[m, 0]
        second_ref[...] = moments[m, 1]
        ratio = ratios[m].reshape(RANK, HD)

        def product(k, total):
            rows = basis[k, :, :, m * RANK : (m + 1) * RANK].reshape(ROWS, RANK)
            update = jnp.dot(rows, ratio, preferred_element_type=F32)
            held[k] = update
            return total + jnp.sum((update * update).reshape(ROWS // 8, 8, HD), axis=0)

        total = lax.fori_loop(0, FN, product, jnp.zeros((8, HD), F32), unroll=2)
        scale = 1.0 / jnp.sqrt(jnp.sum(total) / (D * HD) + norm_floor)

        def scaled(k, _):
            step = held[k] * scale
            old = masters[k, :, m * HD : (m + 1) * HD].astype(F32)
            copy_ref[pl.ds(pl.multiple_of(k * ROWS, ROWS), ROWS), :] = (
                old - step_rate * step
            ).astype(BF)
            return 0

        lax.fori_loop(0, FN, scaled, 0)
        step = held[f] * scale
        step_ref[...] = step
        weight_ref[...] = master[...] - step_rate * step


def body(*args):
    any_space = pl.BlockSpec(memory_space=pl.ANY)
    vmem = pl.BlockSpec(memory_space=pltpu.VMEM)
    dma = pltpu.SemaphoreType.DMA
    basis, masters, ratios, moments = pl.pallas_call(
        exchange,
        name="exchange",
        out_shape=(
            jax.ShapeDtypeStruct((FN, CN, HALF, 2 * RANK), BF),
            jax.ShapeDtypeStruct((FN, ROWS, 2 * HD), BF),
            jax.ShapeDtypeStruct((2, FN, LOW, HD), BF),
            jax.ShapeDtypeStruct((2, 2, LOW, HD), F32),
        ),
        in_specs=[any_space] * len(args),
        out_specs=(vmem,) * 4,
        scratch_shapes=[
            pltpu.VMEM((TOK, HD), BF),
            pltpu.VMEM((SUB, ZN * HD), BF),
            pltpu.VMEM((2, TOK, HD), BF),
            pltpu.VMEM((TOK, HD), BF),
            pltpu.VMEM((TOK, 2 * HD), BF),
            pltpu.VMEM((2 * HD, TOK), BF),
            pltpu.VMEM((2, ROWS, HD), F32),
            pltpu.VMEM((2, 2, LOW, HD), F32),
            pltpu.VMEM((2, LOW, HD), F32),
            pltpu.VMEM((2, SUB, RANK), F32),
            pltpu.VMEM((SUB, RANK), F32),
            pltpu.VMEM((ZN, SUB, RANK), BF),
            pltpu.VMEM((FN, LOW, 2 * HD), F32),
            pltpu.VMEM((FN, LOW, 2 * HD), F32),
            pltpu.VMEM((2, LOW, HD), BF),
            pltpu.VMEM((2, LOW, HD), F32),
            dma((11,)),
            dma((N_SENDS,)),
            dma((N_SENDS,)),
        ],
        compiler_params=pltpu.CompilerParams(
            collective_id=0, has_side_effects=True, vmem_limit_bytes=48 * 1024 * 1024
        ),
    )(*args)
    matrix = jax.ShapeDtypeStruct((ROWS, HD), F32)
    whole = jax.ShapeDtypeStruct((D, HD), BF)
    moment = jax.ShapeDtypeStruct((LOW, HD), F32)
    return pl.pallas_call(
        finish,
        name="finish",
        out_shape=(matrix, matrix, whole, moment, moment) * 2,
        in_specs=[vmem] * 6,
        out_specs=(vmem,) * 10,
        scratch_shapes=[pltpu.VMEM((FN, ROWS, HD), F32)],
        compiler_params=pltpu.CompilerParams(vmem_limit_bytes=48 * 1024 * 1024),
    )(basis, masters, ratios, moments, args[3], args[4])


def solution(mesh):
    torus = Mesh(mesh.devices.reshape(YN, XN, ZN, CN), AXES)
    split = P(FS, TP)
    in_specs = (split,) * 5 + (P(FS, None),) * 2 + (split,) * 4
    out_specs = (split, split, P(None, TP), split, split) * 2
    return jax.shard_map(body, mesh=torus, in_specs=in_specs, out_specs=out_specs, check_vma=False)
```

```python
import jax
import jax.numpy as jnp
from jax import lax
from jax.experimental import pallas as pl
from jax.experimental.pallas import tpu as pltpu
from jax.sharding import Mesh
from jax.sharding import PartitionSpec as P

D = 4096
HD = 128
RANK = 256
YN, XN, ZN, CN = 4, 4, 16, 2
FN = YN * XN
TOK = 1024
SUB = TOK // ZN
ROWS = D // FN
HALF = ROWS // CN
LOW = RANK // FN
AXES = ("y", "x", "z", "c")
FS = ("y", "x")
TP = ("z", "c")

moment_decay = 0.8
square_decay = 0.9
square_floor = 1.0
norm_floor = 0.01
step_rate = 0.01

VMEM_ALL = 67_043_328
MESH_ID = pl.DeviceIdType.MESH
BF = jnp.bfloat16
F32 = jnp.float32

PLANE = sorted(
    [(dy, dx) for dy in range(YN) for dx in range(XN) if (dy, dx) != (0, 0)],
    key=lambda o: -(min(o[0], 4 - o[0]) + min(o[1], 4 - o[1])),
)
ALONG_Z = [8, 7, -7, 6, -6, 5, -5, 4, -4, 3, -3, 2, -2, 1, -1]
Z_FIRST = [6, -6, 3, -3, 1, -1]
Z_RELAY = [(3, (1, -1)), (-3, (-1, 1)), (6, (2, 1, -1)), (-6, (-1, 1))]


class Phases:
    def __init__(self):
        self.open = None

    def __call__(self, name):
        if self.open is not None:
            self.open.__exit__(None, None, None)
        self.open = jax.named_scope(name) if name else None
        if self.open is not None:
            self.open.__enter__()


class Sends:
    def __init__(self, send_sem, recv_sem):
        self.send_sem, self.recv_sem = send_sem, recv_sem
        self.count = 0
        self.started = []

    def take(self):
        self.count += 1
        return self.count - 1

    def start(self, number, src, dst, device):
        copy = pltpu.make_async_remote_copy(
            src_ref=src,
            dst_ref=dst,
            send_sem=self.send_sem.at[number],
            recv_sem=self.recv_sem.at[number],
            device_id=device,
            device_id_type=MESH_ID,
        )
        copy.start()
        self.started.append(copy)

    def landed(self, number, dst, device):
        pltpu.make_async_remote_copy(
            src_ref=dst,
            dst_ref=dst,
            send_sem=self.send_sem.at[number],
            recv_sem=self.recv_sem.at[number],
            device_id=device,
            device_id_type=MESH_ID,
        ).wait_recv()

    def finish(self):
        for copy in self.started:
            copy.wait_send()


def wrap(value, count):
    return lax.rem(value + 2 * count, count)


def plane_gather(sends, piece, me, rows):
    y, x, z, c = me
    half, quarter = rows // 2, rows // 4
    signs = (1, -1)

    def shift(h, first, second):
        d1, d2 = (first, second)
        dy, dx = (d2, d1) if h == 0 else (d1, d2)
        return wrap(y + dy, YN), wrap(x + dx, XN)

    def ref(h, first, second, part=None):
        fy, fx = shift(h, first, second)
        start = h * half + (0 if part is None else part * quarter)
        return piece(fy, fx, start, half if part is None else quarter)

    def dev(h, first, second):
        fy, fx = shift(h, first, second)
        return (fy, fx, z, c)

    part_of = {1: 0, -1: 1}
    both = [(h, s) for h in (0, 1) for s in signs]
    n1 = {k: sends.take() for k in both}
    n1r = {k: sends.take() for k in both}
    n2 = {(h, j, s): sends.take() for j in (0, -1, 1, 2) for h, s in both}
    n2r = {(h, j, s): sends.take() for j in (0, -1, 1, 2) for h, s in both}

    def second_stage(h, j):
        for s in signs:
            sends.start(n2[h, j, s], ref(h, j, 0), ref(h, j, 0), dev(h, 0, s))

    def second_relay(h, j):
        for s in signs:
            sends.landed(n2[h, j, s], ref(h, j, -s), dev(h, 0, s))
            p = part_of[s]
            sends.start(n2r[h, j, s], ref(h, j, -s, p), ref(h, j, -s, p), dev(h, 0, s))

    for h, s in both:
        sends.start(n1[h, s], ref(h, 0, 0), ref(h, 0, 0), dev(h, s, 0))
    for h in (0, 1):
        second_stage(h, 0)
    yield
    for h, s in both:
        sends.landed(n1[h, s], ref(h, -s, 0), dev(h, s, 0))
        p = part_of[s]
        sends.start(n1r[h, s], ref(h, -s, 0, p), ref(h, -s, 0, p), dev(h, s, 0))
        second_stage(h, -s)
    yield
    for h in (0, 1):
        second_relay(h, 0)
    yield
    for h in (0, 1):
        for s in signs:
            p = part_of[s]
            sends.landed(n1r[h, s], ref(h, 2, 0, p), dev(h, s, 0))
        second_stage(h, 2)
    yield
    for j in (-1, 1):
        for h in (0, 1):
            second_relay(h, j)
    yield
    for h in (0, 1):
        second_relay(h, 2)
    yield
    for j in (0, -1, 1, 2):
        for h, s in both:
            p = part_of[s]
            sends.landed(n2r[h, j, s], ref(h, j, 2, p), dev(h, s, 0))


def exchange(
    x_in, qc_in, kc_in, qm_in, km_in, qb_in, kb_in, qf_in, qs_in, kf_in, ks_in,
    basis_out, masters_out, ratios, moments_out,
    basis, masters, xs, xg, cots, cot_other, cot_rel, cot_t, mas, mom, mom_other,
    psend, precv, xb, lowp, lowr, rsend, msend,
    load_sem, store_sem, send_sem, recv_sem,
):
    y, x, z, c = (lax.axis_index(a) for a in AXES)
    me = (y, x, z, c)
    oc = 1 - c
    phase = Phases()
    f = y * XN + x
    partner = (y, x, z, oc)

    phase("enter")
    barrier = pltpu.get_barrier_semaphore()
    near = [(wrap(y + dy, YN), wrap(x + dx, XN), z, c) for dy, dx in PLANE]
    near += [(wrap(y + dy, YN), wrap(x + dx, XN), z, oc) for dy, dx in PLANE]
    near += [partner]
    near += [(y, x, wrap(z + d, ZN), c) for d in ALONG_Z]
    for device in near:
        pl.semaphore_signal(barrier, inc=1, device_id=device, device_id_type=MESH_ID)

    loads = []

    def load(src, dst):
        copy = pltpu.make_async_copy(src, dst, load_sem.at[len(loads)])
        copy.start()
        loads.append(copy)

    mine = pl.ds(pl.multiple_of(c * HALF, HALF), HALF)
    load(x_in, xs)
    load(qb_in.at[mine], basis.at[f, c, :, pl.ds(0, RANK)])
    load(kb_in.at[mine], basis.at[f, c, :, pl.ds(RANK, RANK)])
    load(qc_in, cots.at[0])
    load(kc_in, cots.at[1])
    load(qf_in, mom.at[0, 0])
    load(qs_in, mom.at[0, 1])
    load(kf_in, mom.at[1, 0])
    load(ks_in, mom.at[1, 1])
    load(qm_in, mas.at[0])
    load(km_in, mas.at[1])
    phase("loads")
    for copy in loads:
        copy.wait()
    masters[f, :, 0:HD] = mas[0].astype(BF)
    masters[f, :, HD : 2 * HD] = mas[1].astype(BF)

    sends = Sends(send_sem, recv_sem)
    phase("barrier")
    pl.semaphore_wait(barrier, len(near))

    phase("send_inputs")
    def xslot(zz):
        return xg.at[:, pl.ds(pl.multiple_of(zz * HD, HD), HD)]

    nx = {d: sends.take() for d in ALONG_Z}
    gather_basis = plane_gather(
        sends, lambda fy, fx, s, n: basis.at[fy * XN + fx, c, pl.ds(s, n)], me, HALF
    )
    gather_masters = plane_gather(
        sends, lambda fy, fx, s, n: masters.at[fy * XN + fx, pl.ds(s, n)], me, ROWS
    )
    next(gather_basis)
    for d in ALONG_Z:
        zz = wrap(z + d, ZN)
        rows = xs.at[pl.ds(pl.multiple_of(zz * SUB, SUB), SUB)]
        sends.start(nx[d], rows, xslot(z), (y, x, zz, c))
    n_cot, n_mom = sends.take(), sends.take()
    sends.start(n_cot, cots.at[oc], cot_other, partner)
    sends.start(n_mom, mom.at[oc], mom_other, partner)
    xg[:, pl.ds(pl.multiple_of(z * HD, HD), HD)] = xs[pl.ds(pl.multiple_of(z * SUB, SUB), SUB), :]
    phase("basis_1")
    next(gather_basis)

    phase("cot_rel")
    sends.landed(n_cot, cot_other, partner)
    sends.landed(n_mom, mom_other, partner)
    for o in range(ZN):
        zz = wrap(z - o, ZN)
        rows = pl.ds(pl.multiple_of(zz * SUB, SUB), SUB)
        cot_rel[o * SUB : (o + 1) * SUB, 0:HD] = cots[c, rows, :]
        cot_rel[o * SUB : (o + 1) * SUB, HD : 2 * HD] = cot_other[rows, :]
    phase("basis_23")
    next(gather_basis)
    next(gather_basis)
    phase("cot_t")
    cot_t[...] = cot_rel[...].T
    phase("basis_rest")
    for _ in gather_basis:
        pass
    stores = []

    def store(src, dst):
        copy = pltpu.make_async_copy(src, dst, store_sem.at[len(stores)])
        copy.start()
        stores.append(copy)

    store(basis.at[:, c], basis_out.at[:, c])
    phase("wait_x")
    next(gather_masters)
    for d in ALONG_Z:
        sends.landed(nx[d], xslot(wrap(z - d, ZN)), partner)

    phase("xb")
    part = jnp.zeros((SUB, 2 * RANK), F32)
    for k in range(FN // 2):
        rows = basis[2 * k : 2 * k + 2, c].reshape(2 * HALF, 2 * RANK)
        part += jnp.dot(
            xg[:, k * 2 * HD : (k + 1) * 2 * HD], rows, preferred_element_type=F32
        )
    psend[0] = part[:, :RANK]
    psend[1] = part[:, RANK:]
    n_part = sends.take()
    sends.start(n_part, psend.at[oc], precv, partner)
    n_basis = sends.take()
    phase("d2d_part")
    sends.landed(n_part, precv, partner)
    xb[0] = (psend[c] + precv[...]).astype(BF)

    nz = {}
    for d in Z_FIRST:
        nz[d % ZN] = sends.take()
    for o, hops in Z_RELAY:
        for d in hops:
            nz[(o + d) % ZN] = sends.take()
    seen = set()

    def z_send(o, d):
        sends.start(
            nz[(o + d) % ZN], xb.at[o % ZN], xb.at[(o + d) % ZN], (y, x, wrap(z + d, ZN), c)
        )

    def z_landed(o):
        if o % ZN not in seen:
            seen.add(o % ZN)
            sends.landed(nz[o % ZN], xb.at[o % ZN], partner)

    phase("z_send")
    for d in Z_FIRST:
        z_send(0, d)
    sends.start(n_basis, basis.at[:, c], basis.at[:, c], partner)
    next(gather_masters)
    phase("z_relay1")
    for o, hops in Z_RELAY[:2]:
        z_landed(o)
        for d in hops:
            z_send(o, d)
    phase("z_relay2")
    for o, hops in Z_RELAY[2:]:
        z_landed(o)
        for d in hops:
            z_send(o, d)
    phase("masters")
    next(gather_masters)
    next(gather_masters)
    next(gather_masters)
    phase("z_rest")
    for o in range(1, ZN):
        z_landed(o)
    sends.landed(n_basis, basis.at[:, oc], partner)
    store(basis.at[:, oc], basis_out.at[:, oc])

    phase("low")
    low_t = jnp.dot(cot_t[...], xb[...].reshape(TOK, RANK), preferred_element_type=F32)
    lowp[...] = low_t.T.reshape(FN, LOW, 2 * HD)
    nl = {p: sends.take() for p in PLANE}
    for dy, dx in PLANE:
        ty, tx = wrap(y + dy, YN), wrap(x + dx, XN)
        sends.start(nl[dy, dx], lowp.at[ty * XN + tx], lowr.at[dy * XN + dx], (ty, tx, z, c))
    phase("low_m")
    next(gather_masters)
    phase("low_recv")
    low = lowp[f]
    for dy, dx in PLANE:
        sends.landed(nl[dy, dx], lowr.at[dy * XN + dx], partner)
        low = low + lowr[dy * XN + dx]

    phase("moments")
    nr = {(p, k): sends.take() for p in [(0, 0)] + PLANE for k in (0, 1)}
    n_out = sends.take()
    for k, (first, second) in enumerate(
        ((mom[c, 0], mom[c, 1]), (mom_other[0], mom_other[1]))
    ):
        part = low[:, k * HD : (k + 1) * HD]
        first_new = moment_decay * first + (1.0 - moment_decay) * part
        second_new = square_decay * second + (1.0 - square_decay) * part * part
        rsend[k] = (first_new / jnp.sqrt(second_new + square_floor)).astype(BF)
        if k == 0:
            moments_out[c, 0] = first_new
            moments_out[c, 1] = second_new
        else:
            msend[0] = first_new
            msend[1] = second_new
    ratios[c, f] = rsend[0]
    for dy, dx in PLANE + [(0, 0)]:
        ty, tx = wrap(y + dy, YN), wrap(x + dx, XN)
        for k, core in ((0, c), (1, oc)):
            if k == 0 and (dy, dx) == (0, 0):
                continue
            sends.start(nr[(dy, dx), k], rsend.at[k], ratios.at[c, f], (ty, tx, z, core))
    sends.start(n_out, msend, moments_out.at[c], partner)
    phase("masters_rest")
    for _ in gather_masters:
        pass
    store(masters, masters_out)
    phase("ratio_recv")
    for dy, dx in PLANE + [(0, 0)]:
        sy, sx = wrap(y - dy, YN), wrap(x - dx, XN)
        for k in (0, 1):
            if k == 0 and (dy, dx) == (0, 0):
                continue
            m = c if k == 0 else oc
            sends.landed(nr[(dy, dx), k], ratios.at[m, sy * XN + sx], partner)
    phase("fin")
    sends.landed(n_out, moments_out.at[oc], partner)
    sends.finish()
    for copy in stores:
        copy.wait()
    phase(None)


N_SENDS = 15 + 80 + 2 + 2 + 15 + 15 + 32 + 1


GROUP = 4
GROUPS = FN // GROUP


def finish(
    basis_in, masters_in, ratios_in, moments_in, qm_in, km_in,
    q_step, q_weight, q_copy, q_first, q_second,
    k_step, k_weight, k_copy, k_first, k_second,
    basis, masters, ratios, moments, own, held, steps, weights, copies,
    load_sem, store_sem,
):
    f = lax.axis_index("y") * XN + lax.axis_index("x")
    loads, stores = [], []
    phase = Phases()

    def load(src, dst):
        copy = pltpu.make_async_copy(src, dst, load_sem.at[len(loads)])
        copy.start()
        loads.append(copy)
        return copy

    def store(src, dst):
        copy = pltpu.make_async_copy(src, dst, store_sem.at[len(stores)])
        copy.start()
        stores.append(copy)

    def group(g):
        return pl.ds(g * GROUP, GROUP)

    ratio_load = load(ratios_in, ratios)
    basis_loads = [load(basis_in.at[group(g)], basis.at[group(g)]) for g in range(GROUPS)]
    moments_load = load(moments_in, moments)
    own_loads = [load(qm_in, own.at[0]), load(km_in, own.at[1])]
    masters_loads = [load(masters_in.at[group(g)], masters.at[group(g)]) for g in range(GROUPS)]

    phase("ratio_wait")
    ratio_load.wait()
    ratio = [ratios[m].reshape(RANK, HD) for m in range(2)]
    phase("product")
    totals = [jnp.zeros((8, HD), F32) for _ in range(2)]
    for g in range(GROUPS):
        basis_loads[g].wait()
        for k in range(g * GROUP, (g + 1) * GROUP):
            for m in range(2):
                rows = basis[k, :, :, m * RANK : (m + 1) * RANK].reshape(ROWS, RANK)
                update = jnp.dot(rows, ratio[m], preferred_element_type=F32)
                held[m, k] = update
                totals[m] += jnp.sum((update * update).reshape(ROWS // 8, 8, HD), axis=0)
    phase("scale")
    moments_load.wait()
    for m, refs in enumerate(((q_first, q_second), (k_first, k_second))):
        for i in range(2):
            store(moments.at[m, i], refs[i])
    scales = [1.0 / jnp.sqrt(jnp.sum(t) / (D * HD) + norm_floor) for t in totals]
    for m, (step_ref, weight_ref) in enumerate(((q_step, q_weight), (k_step, k_weight))):
        own_loads[m].wait()
        step = held[m, f] * scales[m]
        steps[m] = step
        weights[m] = own[m] - step_rate * step
        store(steps.at[m], step_ref)
        store(weights.at[m], weight_ref)
    phase("copies")
    for g in range(GROUPS):
        masters_loads[g].wait()
        for m, copy_ref in enumerate((q_copy, k_copy)):
            for k in range(g * GROUP, (g + 1) * GROUP):
                old = masters[k, :, m * HD : (m + 1) * HD].astype(F32)
                copies[m, k * ROWS : (k + 1) * ROWS] = (
                    old - step_rate * (held[m, k] * scales[m])
                ).astype(BF)
            rows = pl.ds(g * GROUP * ROWS, GROUP * ROWS)
            store(copies.at[m, rows], copy_ref.at[rows])
    phase("drain")
    for copy in stores:
        copy.wait()
    phase(None)


def body(*args):
    any_space = pl.BlockSpec(memory_space=pl.ANY)
    vmem = pl.BlockSpec(memory_space=pltpu.VMEM)
    dma = pltpu.SemaphoreType.DMA
    basis, masters, ratios, moments = pl.pallas_call(
        exchange,
        name="exchange",
        out_shape=(
            jax.ShapeDtypeStruct((FN, CN, HALF, 2 * RANK), BF),
            jax.ShapeDtypeStruct((FN, ROWS, 2 * HD), BF),
            jax.ShapeDtypeStruct((2, FN, LOW, HD), BF),
            jax.ShapeDtypeStruct((2, 2, LOW, HD), F32),
        ),
        in_specs=[any_space] * len(args),
        out_specs=(any_space, any_space, vmem, vmem),
        scratch_shapes=[
            pltpu.VMEM((FN, CN, HALF, 2 * RANK), BF),
            pltpu.VMEM((FN, ROWS, 2 * HD), BF),
            pltpu.VMEM((TOK, HD), BF),
            pltpu.VMEM((SUB, ZN * HD), BF),
            pltpu.VMEM((2, TOK, HD), BF),
            pltpu.VMEM((TOK, HD), BF),
            pltpu.VMEM((TOK, 2 * HD), BF),
            pltpu.VMEM((2 * HD, TOK), BF),
            pltpu.VMEM((2, ROWS, HD), F32),
            pltpu.VMEM((2, 2, LOW, HD), F32),
            pltpu.VMEM((2, LOW, HD), F32),
            pltpu.VMEM((2, SUB, RANK), F32),
            pltpu.VMEM((SUB, RANK), F32),
            pltpu.VMEM((ZN, SUB, RANK), BF),
            pltpu.VMEM((FN, LOW, 2 * HD), F32),
            pltpu.VMEM((FN, LOW, 2 * HD), F32),
            pltpu.VMEM((2, LOW, HD), BF),
            pltpu.VMEM((2, LOW, HD), F32),
            dma((11,)),
            dma((3,)),
            dma((N_SENDS,)),
            dma((N_SENDS,)),
        ],
        compiler_params=pltpu.CompilerParams(
            collective_id=0, has_side_effects=True, vmem_limit_bytes=VMEM_ALL
        ),
    )(*args)
    matrix = jax.ShapeDtypeStruct((ROWS, HD), F32)
    whole = jax.ShapeDtypeStruct((D, HD), BF)
    moment = jax.ShapeDtypeStruct((LOW, HD), F32)
    return pl.pallas_call(
        finish,
        name="finish",
        out_shape=(matrix, matrix, whole, moment, moment) * 2,
        in_specs=[any_space] * 6,
        out_specs=(any_space,) * 10,
        scratch_shapes=[
            pltpu.VMEM((FN, CN, HALF, 2 * RANK), BF),
            pltpu.VMEM((FN, ROWS, 2 * HD), BF),
            pltpu.VMEM((2, FN, LOW, HD), BF),
            pltpu.VMEM((2, 2, LOW, HD), F32),
            pltpu.VMEM((2, ROWS, HD), F32),
            pltpu.VMEM((2, FN, ROWS, HD), F32),
            pltpu.VMEM((2, ROWS, HD), F32),
            pltpu.VMEM((2, ROWS, HD), F32),
            pltpu.VMEM((2, D, HD), BF),
            dma((4 + 2 * GROUPS,)),
            dma((8 + 2 * GROUPS,)),
        ],
        compiler_params=pltpu.CompilerParams(vmem_limit_bytes=VMEM_ALL),
    )(basis, masters, ratios, moments, args[3], args[4])


def solution(mesh):
    torus = Mesh(mesh.devices.reshape(YN, XN, ZN, CN), AXES)
    split = P(FS, TP)
    in_specs = (split,) * 5 + (P(FS, None),) * 2 + (split,) * 4
    out_specs = (split, split, P(None, TP), split, split) * 2
    return jax.shard_map(body, mesh=torus, in_specs=in_specs, out_specs=out_specs, check_vma=False)
```

```python
import jax
import jax.numpy as jnp
from jax import lax
from jax.experimental import pallas as pl
from jax.experimental.pallas import tpu as pltpu
from jax.sharding import Mesh
from jax.sharding import PartitionSpec as P

D = 4096
HD = 128
RANK = 256
YN, XN, ZN, CN = 4, 4, 16, 2
FN = YN * XN
TOK = 1024
SUB = TOK // ZN
ROWS = D // FN
HALF = ROWS // CN
LOW = RANK // FN
AXES = ("y", "x", "z", "c")
FS = ("y", "x")
TP = ("z", "c")

moment_decay = 0.8
square_decay = 0.9
square_floor = 1.0
norm_floor = 0.01
step_rate = 0.01

VMEM_GRANT = 20 * 1024 * 1024
MESH_ID = pl.DeviceIdType.MESH
BF = jnp.bfloat16
F32 = jnp.float32

PLANE = sorted(
    [(dy, dx) for dy in range(YN) for dx in range(XN) if (dy, dx) != (0, 0)],
    key=lambda o: -(min(o[0], 4 - o[0]) + min(o[1], 4 - o[1])),
)
ALONG_Z = [8, 7, -7, 6, -6, 5, -5, 4, -4, 3, -3, 2, -2, 1, -1]
Z_FIRST = [6, -6, 3, -3, 1, -1]
Z_RELAY = [(3, (1, -1)), (-3, (-1, 1)), (6, (2, 1, -1)), (-6, (-1, 1))]


class Phases:
    def __init__(self):
        self.open = None

    def __call__(self, name):
        if self.open is not None:
            self.open.__exit__(None, None, None)
        self.open = jax.named_scope(name) if name else None
        if self.open is not None:
            self.open.__enter__()


class Sends:
    def __init__(self, send_sem, recv_sem):
        self.send_sem, self.recv_sem = send_sem, recv_sem
        self.count = 0
        self.started = []

    def take(self):
        self.count += 1
        return self.count - 1

    def start(self, number, src, dst, device):
        copy = pltpu.make_async_remote_copy(
            src_ref=src,
            dst_ref=dst,
            send_sem=self.send_sem.at[number],
            recv_sem=self.recv_sem.at[number],
            device_id=device,
            device_id_type=MESH_ID,
        )
        copy.start()
        self.started.append(copy)

    def landed(self, number, dst, device):
        pltpu.make_async_remote_copy(
            src_ref=dst,
            dst_ref=dst,
            send_sem=self.send_sem.at[number],
            recv_sem=self.recv_sem.at[number],
            device_id=device,
            device_id_type=MESH_ID,
        ).wait_recv()

    def finish(self):
        for copy in self.started:
            copy.wait_send()


def wrap(value, count):
    return lax.rem(value + 2 * count, count)


def plane_gather(sends, piece, me, rows):
    y, x, z, c = me
    half, quarter = rows // 2, rows // 4
    signs = (1, -1)

    def shift(h, first, second):
        d1, d2 = (first, second)
        dy, dx = (d2, d1) if h == 0 else (d1, d2)
        return wrap(y + dy, YN), wrap(x + dx, XN)

    def ref(h, first, second, part=None):
        fy, fx = shift(h, first, second)
        start = h * half + (0 if part is None else part * quarter)
        return piece(fy, fx, start, half if part is None else quarter)

    def dev(h, first, second):
        fy, fx = shift(h, first, second)
        return (fy, fx, z, c)

    part_of = {1: 0, -1: 1}
    both = [(h, s) for h in (0, 1) for s in signs]
    n1 = {k: sends.take() for k in both}
    n1r = {k: sends.take() for k in both}
    n2 = {(h, j, s): sends.take() for j in (0, -1, 1, 2) for h, s in both}
    n2r = {(h, j, s): sends.take() for j in (0, -1, 1, 2) for h, s in both}

    def second_stage(h, j):
        for s in signs:
            sends.start(n2[h, j, s], ref(h, j, 0), ref(h, j, 0), dev(h, 0, s))

    def second_relay(h, j):
        for s in signs:
            sends.landed(n2[h, j, s], ref(h, j, -s), dev(h, 0, s))
            p = part_of[s]
            sends.start(n2r[h, j, s], ref(h, j, -s, p), ref(h, j, -s, p), dev(h, 0, s))

    for h, s in both:
        sends.start(n1[h, s], ref(h, 0, 0), ref(h, 0, 0), dev(h, s, 0))
    for h in (0, 1):
        second_stage(h, 0)
    yield
    for h, s in both:
        sends.landed(n1[h, s], ref(h, -s, 0), dev(h, s, 0))
        p = part_of[s]
        sends.start(n1r[h, s], ref(h, -s, 0, p), ref(h, -s, 0, p), dev(h, s, 0))
        second_stage(h, -s)
    yield
    for h in (0, 1):
        second_relay(h, 0)
    yield
    for h in (0, 1):
        for s in signs:
            p = part_of[s]
            sends.landed(n1r[h, s], ref(h, 2, 0, p), dev(h, s, 0))
        second_stage(h, 2)
    yield
    for j in (-1, 1):
        for h in (0, 1):
            second_relay(h, j)
    yield
    for h in (0, 1):
        second_relay(h, 2)
    yield
    for j in (0, -1, 1, 2):
        for h, s in both:
            p = part_of[s]
            sends.landed(n2r[h, j, s], ref(h, j, 2, p), dev(h, s, 0))


def exchange(
    x_in, qc_in, kc_in, qm_in, km_in, qb_in, kb_in, qf_in, qs_in, kf_in, ks_in,
    basis, masters, ratios, moments_out, mas,
    xs, xg, cots, cot_other, cot_rel, cot_t, mom, mom_other,
    psend, precv, xb, lowp, lowr, rsend, msend,
    load_sem, send_sem, recv_sem,
):
    y, x, z, c = (lax.axis_index(a) for a in AXES)
    me = (y, x, z, c)
    oc = 1 - c
    phase = Phases()
    f = y * XN + x
    partner = (y, x, z, oc)

    phase("enter")
    barrier = pltpu.get_barrier_semaphore()
    near = [(wrap(y + dy, YN), wrap(x + dx, XN), z, c) for dy, dx in PLANE]
    near += [(wrap(y + dy, YN), wrap(x + dx, XN), z, oc) for dy, dx in PLANE]
    near += [partner]
    near += [(y, x, wrap(z + d, ZN), c) for d in ALONG_Z]
    for device in near:
        pl.semaphore_signal(barrier, inc=1, device_id=device, device_id_type=MESH_ID)

    loads = []

    def load(src, dst):
        copy = pltpu.make_async_copy(src, dst, load_sem.at[len(loads)])
        copy.start()
        loads.append(copy)

    mine = pl.ds(pl.multiple_of(c * HALF, HALF), HALF)
    load(x_in, xs)
    load(qb_in.at[mine], basis.at[f, c, :, pl.ds(0, RANK)])
    load(kb_in.at[mine], basis.at[f, c, :, pl.ds(RANK, RANK)])
    load(qc_in, cots.at[0])
    load(kc_in, cots.at[1])
    load(qf_in, mom.at[0, 0])
    load(qs_in, mom.at[0, 1])
    load(kf_in, mom.at[1, 0])
    load(ks_in, mom.at[1, 1])
    load(qm_in, mas.at[0])
    load(km_in, mas.at[1])
    phase("loads")
    for copy in loads:
        copy.wait()
    masters[f, :, 0:HD] = mas[0].astype(BF)
    masters[f, :, HD : 2 * HD] = mas[1].astype(BF)

    sends = Sends(send_sem, recv_sem)
    phase("barrier")
    pl.semaphore_wait(barrier, len(near))

    phase("send_inputs")
    def xslot(zz):
        return xg.at[:, pl.ds(pl.multiple_of(zz * HD, HD), HD)]

    nx = {d: sends.take() for d in ALONG_Z}
    gather_basis = plane_gather(
        sends, lambda fy, fx, s, n: basis.at[fy * XN + fx, c, pl.ds(s, n)], me, HALF
    )
    gather_masters = plane_gather(
        sends, lambda fy, fx, s, n: masters.at[fy * XN + fx, pl.ds(s, n)], me, ROWS
    )
    next(gather_basis)
    for d in ALONG_Z:
        zz = wrap(z + d, ZN)
        rows = xs.at[pl.ds(pl.multiple_of(zz * SUB, SUB), SUB)]
        sends.start(nx[d], rows, xslot(z), (y, x, zz, c))
    n_cot, n_mom = sends.take(), sends.take()
    sends.start(n_cot, cots.at[oc], cot_other, partner)
    sends.start(n_mom, mom.at[oc], mom_other, partner)
    xg[:, pl.ds(pl.multiple_of(z * HD, HD), HD)] = xs[pl.ds(pl.multiple_of(z * SUB, SUB), SUB), :]
    phase("basis_1")
    next(gather_basis)

    phase("cot_rel")
    sends.landed(n_cot, cot_other, partner)
    sends.landed(n_mom, mom_other, partner)
    for o in range(ZN):
        zz = wrap(z - o, ZN)
        rows = pl.ds(pl.multiple_of(zz * SUB, SUB), SUB)
        cot_rel[o * SUB : (o + 1) * SUB, 0:HD] = cots[c, rows, :]
        cot_rel[o * SUB : (o + 1) * SUB, HD : 2 * HD] = cot_other[rows, :]
    phase("basis_23")
    next(gather_basis)
    next(gather_basis)
    phase("cot_t")
    cot_t[...] = cot_rel[...].T
    phase("basis_rest")
    for _ in gather_basis:
        pass
    phase("wait_x")
    next(gather_masters)
    for d in ALONG_Z:
        sends.landed(nx[d], xslot(wrap(z - d, ZN)), partner)

    phase("xb")
    part = jnp.zeros((SUB, 2 * RANK), F32)
    for k in range(FN // 2):
        rows = basis[2 * k : 2 * k + 2, c].reshape(2 * HALF, 2 * RANK)
        part += jnp.dot(
            xg[:, k * 2 * HD : (k + 1) * 2 * HD], rows, preferred_element_type=F32
        )
    psend[0] = part[:, :RANK]
    psend[1] = part[:, RANK:]
    n_part = sends.take()
    sends.start(n_part, psend.at[oc], precv, partner)
    n_basis = sends.take()
    phase("d2d_part")
    sends.landed(n_part, precv, partner)
    xb[0] = (psend[c] + precv[...]).astype(BF)

    nz = {}
    for d in Z_FIRST:
        nz[d % ZN] = sends.take()
    for o, hops in Z_RELAY:
        for d in hops:
            nz[(o + d) % ZN] = sends.take()
    seen = set()

    def z_send(o, d):
        sends.start(
            nz[(o + d) % ZN], xb.at[o % ZN], xb.at[(o + d) % ZN], (y, x, wrap(z + d, ZN), c)
        )

    def z_landed(o):
        if o % ZN not in seen:
            seen.add(o % ZN)
            sends.landed(nz[o % ZN], xb.at[o % ZN], partner)

    phase("z_send")
    for d in Z_FIRST:
        z_send(0, d)
    sends.start(n_basis, basis.at[:, c], basis.at[:, c], partner)
    next(gather_masters)
    phase("z_relay1")
    for o, hops in Z_RELAY[:2]:
        z_landed(o)
        for d in hops:
            z_send(o, d)
    phase("z_relay2")
    for o, hops in Z_RELAY[2:]:
        z_landed(o)
        for d in hops:
            z_send(o, d)
    phase("masters")
    next(gather_masters)
    next(gather_masters)
    next(gather_masters)
    phase("z_rest")
    for o in range(1, ZN):
        z_landed(o)
    sends.landed(n_basis, basis.at[:, oc], partner)

    phase("low")
    low_t = jnp.dot(cot_t[...], xb[...].reshape(TOK, RANK), preferred_element_type=F32)
    lowp[...] = low_t.T.reshape(FN, LOW, 2 * HD)
    nl = {p: sends.take() for p in PLANE}
    for dy, dx in PLANE:
        ty, tx = wrap(y + dy, YN), wrap(x + dx, XN)
        sends.start(nl[dy, dx], lowp.at[ty * XN + tx], lowr.at[dy * XN + dx], (ty, tx, z, c))
    phase("low_m")
    next(gather_masters)
    phase("low_recv")
    low = lowp[f]
    for dy, dx in PLANE:
        sends.landed(nl[dy, dx], lowr.at[dy * XN + dx], partner)
        low = low + lowr[dy * XN + dx]

    phase("moments")
    nr = {(p, k): sends.take() for p in [(0, 0)] + PLANE for k in (0, 1)}
    n_out = sends.take()
    for k, (first, second) in enumerate(
        ((mom[c, 0], mom[c, 1]), (mom_other[0], mom_other[1]))
    ):
        part = low[:, k * HD : (k + 1) * HD]
        first_new = moment_decay * first + (1.0 - moment_decay) * part
        second_new = square_decay * second + (1.0 - square_decay) * part * part
        rsend[k] = (first_new / jnp.sqrt(second_new + square_floor)).astype(BF)
        if k == 0:
            moments_out[c, 0] = first_new
            moments_out[c, 1] = second_new
        else:
            msend[0] = first_new
            msend[1] = second_new
    ratios[c, f] = rsend[0]
    for dy, dx in PLANE + [(0, 0)]:
        ty, tx = wrap(y + dy, YN), wrap(x + dx, XN)
        for k, core in ((0, c), (1, oc)):
            if k == 0 and (dy, dx) == (0, 0):
                continue
            sends.start(nr[(dy, dx), k], rsend.at[k], ratios.at[c, f], (ty, tx, z, core))
    sends.start(n_out, msend, moments_out.at[c], partner)
    phase("masters_rest")
    for _ in gather_masters:
        pass
    phase("ratio_recv")
    for dy, dx in PLANE + [(0, 0)]:
        sy, sx = wrap(y - dy, YN), wrap(x - dx, XN)
        for k in (0, 1):
            if k == 0 and (dy, dx) == (0, 0):
                continue
            m = c if k == 0 else oc
            sends.landed(nr[(dy, dx), k], ratios.at[m, sy * XN + sx], partner)
    phase("fin")
    sends.landed(n_out, moments_out.at[oc], partner)
    sends.finish()
    phase(None)


N_SENDS = 15 + 80 + 2 + 2 + 15 + 15 + 32 + 1


GROUP = 4
GROUPS = FN // GROUP


def finish(
    basis, masters, ratios, moments, own,
    q_step, q_weight, q_copy, q_first, q_second,
    k_step, k_weight, k_copy, k_first, k_second,
    held, steps, weights, copies,
    store_sem,
):
    f = lax.axis_index("y") * XN + lax.axis_index("x")
    stores = []
    phase = Phases()

    def store(src, dst):
        copy = pltpu.make_async_copy(src, dst, store_sem.at[len(stores)])
        copy.start()
        stores.append(copy)

    phase("product")
    ratio = [ratios[m].reshape(RANK, HD) for m in range(2)]
    totals = [jnp.zeros((8, HD), F32) for _ in range(2)]
    for g in range(GROUPS):
        for k in range(g * GROUP, (g + 1) * GROUP):
            for m in range(2):
                rows = basis[k, :, :, m * RANK : (m + 1) * RANK].reshape(ROWS, RANK)
                update = jnp.dot(rows, ratio[m], preferred_element_type=F32)
                held[m, k] = update
                totals[m] += jnp.sum((update * update).reshape(ROWS // 8, 8, HD), axis=0)
    phase("scale")
    for m, refs in enumerate(((q_first, q_second), (k_first, k_second))):
        for i in range(2):
            store(moments.at[m, i], refs[i])
    scales = [1.0 / jnp.sqrt(jnp.sum(t) / (D * HD) + norm_floor) for t in totals]
    for m, (step_ref, weight_ref) in enumerate(((q_step, q_weight), (k_step, k_weight))):
        step = held[m, f] * scales[m]
        steps[m] = step
        weights[m] = own[m] - step_rate * step
        store(steps.at[m], step_ref)
        store(weights.at[m], weight_ref)
    phase("copies")
    for g in range(GROUPS):
        for m, copy_ref in enumerate((q_copy, k_copy)):
            for k in range(g * GROUP, (g + 1) * GROUP):
                old = masters[k, :, m * HD : (m + 1) * HD].astype(F32)
                copies[m, k * ROWS : (k + 1) * ROWS] = (
                    old - step_rate * (held[m, k] * scales[m])
                ).astype(BF)
            rows = pl.ds(g * GROUP * ROWS, GROUP * ROWS)
            store(copies.at[m, rows], copy_ref.at[rows])
    phase("drain")
    for copy in stores:
        copy.wait()
    phase(None)


def body(*args):
    hbm = pl.BlockSpec(memory_space=pltpu.HBM)
    vmem = pl.BlockSpec(memory_space=pltpu.VMEM)
    dma = pltpu.SemaphoreType.DMA
    handed = pl.pallas_call(
        exchange,
        name="exchange",
        out_shape=(
            jax.ShapeDtypeStruct((FN, CN, HALF, 2 * RANK), BF),
            jax.ShapeDtypeStruct((FN, ROWS, 2 * HD), BF),
            jax.ShapeDtypeStruct((2, FN, LOW, HD), BF),
            jax.ShapeDtypeStruct((2, 2, LOW, HD), F32),
            jax.ShapeDtypeStruct((2, ROWS, HD), F32),
        ),
        in_specs=[hbm] * len(args),
        out_specs=(vmem,) * 5,
        scratch_shapes=[
            pltpu.VMEM((TOK, HD), BF),
            pltpu.VMEM((SUB, ZN * HD), BF),
            pltpu.VMEM((2, TOK, HD), BF),
            pltpu.VMEM((TOK, HD), BF),
            pltpu.VMEM((TOK, 2 * HD), BF),
            pltpu.VMEM((2 * HD, TOK), BF),
            pltpu.VMEM((2, 2, LOW, HD), F32),
            pltpu.VMEM((2, LOW, HD), F32),
            pltpu.VMEM((2, SUB, RANK), F32),
            pltpu.VMEM((SUB, RANK), F32),
            pltpu.VMEM((ZN, SUB, RANK), BF),
            pltpu.VMEM((FN, LOW, 2 * HD), F32),
            pltpu.VMEM((FN, LOW, 2 * HD), F32),
            pltpu.VMEM((2, LOW, HD), BF),
            pltpu.VMEM((2, LOW, HD), F32),
            dma((11,)),
            dma((N_SENDS,)),
            dma((N_SENDS,)),
        ],
        compiler_params=pltpu.CompilerParams(
            collective_id=0, has_side_effects=True, vmem_limit_bytes=VMEM_GRANT
        ),
    )(*(pltpu.with_memory_space_constraint(a, pltpu.HBM) for a in args))
    matrix = jax.ShapeDtypeStruct((ROWS, HD), F32)
    whole = jax.ShapeDtypeStruct((D, HD), BF)
    moment = jax.ShapeDtypeStruct((LOW, HD), F32)
    return pl.pallas_call(
        finish,
        name="finish",
        out_shape=(matrix, matrix, whole, moment, moment) * 2,
        in_specs=[vmem] * 5,
        out_specs=(hbm,) * 10,
        scratch_shapes=[
            pltpu.VMEM((2, FN, ROWS, HD), F32),
            pltpu.VMEM((2, ROWS, HD), F32),
            pltpu.VMEM((2, ROWS, HD), F32),
            pltpu.VMEM((2, D, HD), BF),
            dma((8 + 2 * GROUPS,)),
        ],
        compiler_params=pltpu.CompilerParams(vmem_limit_bytes=VMEM_GRANT),
    )(*handed)


def solution(mesh):
    torus = Mesh(mesh.devices.reshape(YN, XN, ZN, CN), AXES)
    split = P(FS, TP)
    in_specs = (split,) * 5 + (P(FS, None),) * 2 + (split,) * 4
    out_specs = (split, split, P(None, TP), split, split) * 2
    return jax.shard_map(body, mesh=torus, in_specs=in_specs, out_specs=out_specs, check_vma=False)
```

```python
import jax
import jax.numpy as jnp
from jax import lax
from jax.experimental import pallas as pl
from jax.experimental.pallas import tpu as pltpu
from jax.sharding import Mesh
from jax.sharding import PartitionSpec as P

D = 4096
HD = 128
RANK = 256
YN, XN, ZN, CN = 4, 4, 16, 2
FN = YN * XN
TOK = 1024
SUB = TOK // ZN
ROWS = D // FN
HALF = ROWS // CN
LOW = RANK // FN
AXES = ("y", "x", "z", "c")
FS = ("y", "x")
TP = ("z", "c")

moment_decay = 0.8
square_decay = 0.9
square_floor = 1.0
norm_floor = 0.01
step_rate = 0.01

VMEM_GRANT = 20 * 1024 * 1024
MESH_ID = pl.DeviceIdType.MESH
BF = jnp.bfloat16
F32 = jnp.float32

PLANE = sorted(
    [(dy, dx) for dy in range(YN) for dx in range(XN) if (dy, dx) != (0, 0)],
    key=lambda o: -(min(o[0], 4 - o[0]) + min(o[1], 4 - o[1])),
)
ALONG_Z = [8, 7, -7, 6, -6, 5, -5, 4, -4, 3, -3, 2, -2, 1, -1]
Z_FIRST = [6, -6, 3, -3, 1, -1]
Z_RELAY = [(3, (1, -1)), (-3, (-1, 1)), (6, (2, 1, -1)), (-6, (-1, 1))]


class Phases:
    def __init__(self):
        self.open = None

    def __call__(self, name):
        if self.open is not None:
            self.open.__exit__(None, None, None)
        self.open = jax.named_scope(name) if name else None
        if self.open is not None:
            self.open.__enter__()


class Sends:
    def __init__(self, send_sem, recv_sem):
        self.send_sem, self.recv_sem = send_sem, recv_sem
        self.sent = self.received = 0
        self.open = []

    def sent_group(self, whole):
        self.open.append((self.sent, whole))
        self.sent += 1
        return self.sent - 1

    def received_group(self):
        self.received += 1
        return self.received - 1

    def start(self, sent, received, src, dst, device):
        pltpu.make_async_remote_copy(
            src_ref=src,
            dst_ref=dst,
            send_sem=self.send_sem.at[sent],
            recv_sem=self.recv_sem.at[received],
            device_id=device,
            device_id_type=MESH_ID,
        ).start()

    def whole(self, sent, received, ref, device):
        return pltpu.make_async_remote_copy(
            src_ref=ref,
            dst_ref=ref,
            send_sem=self.send_sem.at[sent],
            recv_sem=self.recv_sem.at[received],
            device_id=device,
            device_id_type=MESH_ID,
        )

    def landed(self, received, ref, device):
        self.whole(0, received, ref, device).wait_recv()

    def finish(self, device):
        for group, ref in self.open:
            self.whole(group, 0, ref, device).wait_send()


def wrap(value, count):
    return lax.rem(value + 2 * count, count)


def plane_gather(sends, piece, many, me, rows):
    y, x, z, c = me
    half, quarter = rows // 2, rows // 4
    signs = (1, -1)

    def shift(h, first, second):
        d1, d2 = (first, second)
        dy, dx = (d2, d1) if h == 0 else (d1, d2)
        return wrap(y + dy, YN), wrap(x + dx, XN)

    def ref(h, first, second, part=None):
        fy, fx = shift(h, first, second)
        start = h * half + (0 if part is None else part * quarter)
        return piece(fy, fx, start, half if part is None else quarter)

    def dev(h, first, second):
        fy, fx = shift(h, first, second)
        return (fy, fx, z, c)

    part_of = {1: 0, -1: 1}
    halves = (0, 1)
    sent = sends.sent_group(many(FN - 1, 0, rows))
    n1 = {h: sends.received_group() for h in halves}
    n1r = {h: sends.received_group() for h in halves}
    n2 = {(h, j): sends.received_group() for j in (0, -1, 1, 2) for h in halves}
    n2r = sends.received_group()
    me_dev = dev(0, 1, 0)

    def go(number, source, target):
        sends.start(sent, number, source, source, target)

    def second_stage(h, j):
        for s in signs:
            go(n2[h, j], ref(h, j, 0), dev(h, 0, s))

    def second_relay(h, j):
        sends.landed(n2[h, j], many(2, 0, half), me_dev)
        for s in signs:
            go(n2r, ref(h, j, -s, part_of[s]), dev(h, 0, s))

    for h in halves:
        for s in signs:
            go(n1[h], ref(h, 0, 0), dev(h, s, 0))
    for h in halves:
        second_stage(h, 0)
    yield
    for h in halves:
        sends.landed(n1[h], many(2, 0, half), me_dev)
        for s in signs:
            go(n1r[h], ref(h, -s, 0, part_of[s]), dev(h, s, 0))
    for h in halves:
        second_stage(h, -1)
        second_stage(h, 1)
    yield
    for h in halves:
        second_relay(h, 0)
    yield
    for h in halves:
        sends.landed(n1r[h], many(1, 0, half), me_dev)
        second_stage(h, 2)
    yield
    for j in (-1, 1):
        for h in halves:
            second_relay(h, j)
    yield
    for h in halves:
        second_relay(h, 2)
    yield
    sends.landed(n2r, many(8, 0, half), me_dev)


def exchange(
    x_in, qc_in, kc_in, qm_in, km_in, qb_in, kb_in, qf_in, qs_in, kf_in, ks_in,
    basis, masters, ratios, moments_out, mas,
    xs, xg, cots, cot_other, cot_rel, cot_t, mom, mom_other,
    psend, precv, xb, lowf, lowp, lowr, rsend, msend,
    load_sem, send_sem, recv_sem,
):
    y, x, z, c = (lax.axis_index(a) for a in AXES)
    me = (y, x, z, c)
    oc = 1 - c
    phase = Phases()
    f = y * XN + x
    partner = (y, x, z, oc)

    phase("enter")
    barrier = pltpu.get_barrier_semaphore()
    near = [(wrap(y + dy, YN), wrap(x + dx, XN), z, c) for dy, dx in PLANE]
    near += [(wrap(y + dy, YN), wrap(x + dx, XN), z, oc) for dy, dx in PLANE]
    near += [partner]
    near += [(y, x, wrap(z + d, ZN), c) for d in ALONG_Z]
    for device in near:
        pl.semaphore_signal(barrier, inc=1, device_id=device, device_id_type=MESH_ID)

    loads = []

    def load(src, dst):
        copy = pltpu.make_async_copy(src, dst, load_sem.at[len(loads)])
        copy.start()
        loads.append(copy)

    mine = pl.ds(pl.multiple_of(c * HALF, HALF), HALF)
    load(x_in, xs)
    load(qb_in.at[mine], basis.at[f, c, :, pl.ds(0, RANK)])
    load(kb_in.at[mine], basis.at[f, c, :, pl.ds(RANK, RANK)])
    load(qc_in, cots.at[0])
    load(kc_in, cots.at[1])
    load(qf_in, mom.at[0, 0])
    load(qs_in, mom.at[0, 1])
    load(kf_in, mom.at[1, 0])
    load(ks_in, mom.at[1, 1])
    load(qm_in, mas.at[0])
    load(km_in, mas.at[1])
    phase("loads")
    for copy in loads:
        copy.wait()
    masters[f, :, 0:HD] = mas[0].astype(BF)
    masters[f, :, HD : 2 * HD] = mas[1].astype(BF)

    sends = Sends(send_sem, recv_sem)
    phase("barrier")
    pl.semaphore_wait(barrier, len(near))

    phase("send_inputs")
    def xslot(zz):
        return xg.at[:, pl.ds(pl.multiple_of(zz * HD, HD), HD)]

    several = xs.at[pl.ds(0, (ZN - 1) * SUB)]
    sent_x, got_x = sends.sent_group(several), sends.received_group()
    gather_basis = plane_gather(
        sends,
        lambda fy, fx, s, n: basis.at[fy * XN + fx, c, pl.ds(s, n)],
        lambda k, s, n: basis.at[pl.ds(0, k), 0, pl.ds(s, n)],
        me,
        HALF,
    )
    gather_masters = plane_gather(
        sends,
        lambda fy, fx, s, n: masters.at[fy * XN + fx, pl.ds(s, n)],
        lambda k, s, n: masters.at[pl.ds(0, k), pl.ds(s, n)],
        me,
        ROWS,
    )
    next(gather_basis)
    for d in ALONG_Z:
        zz = wrap(z + d, ZN)
        rows = xs.at[pl.ds(pl.multiple_of(zz * SUB, SUB), SUB)]
        sends.start(sent_x, got_x, rows, xslot(z), (y, x, zz, c))

    def swap(src, dst):
        received = sends.received_group()
        sends.start(sends.sent_group(src), received, src, dst, partner)
        return received

    n_cot = swap(cots.at[oc], cot_other)
    n_mom = swap(mom.at[oc], mom_other)
    xg[:, pl.ds(pl.multiple_of(z * HD, HD), HD)] = xs[pl.ds(pl.multiple_of(z * SUB, SUB), SUB), :]
    phase("basis_1")
    next(gather_basis)

    phase("cot_rel")
    sends.landed(n_cot, cot_other, partner)
    sends.landed(n_mom, mom_other, partner)
    for o in range(ZN):
        zz = wrap(z - o, ZN)
        rows = pl.ds(pl.multiple_of(zz * SUB, SUB), SUB)
        cot_rel[o * SUB : (o + 1) * SUB, 0:HD] = cots[c, rows, :]
        cot_rel[o * SUB : (o + 1) * SUB, HD : 2 * HD] = cot_other[rows, :]
    phase("basis_23")
    next(gather_basis)
    next(gather_basis)
    phase("cot_t")
    cot_t[...] = cot_rel[...].T
    phase("basis_rest")
    for _ in gather_basis:
        pass
    phase("wait_x")
    next(gather_masters)
    sends.landed(got_x, several, partner)

    phase("xb")
    part = jnp.zeros((SUB, 2 * RANK), F32)
    for k in range(FN // 2):
        rows = basis[2 * k : 2 * k + 2, c].reshape(2 * HALF, 2 * RANK)
        part += jnp.dot(
            xg[:, k * 2 * HD : (k + 1) * 2 * HD], rows, preferred_element_type=F32
        )
    psend[0] = part[:, :RANK]
    psend[1] = part[:, RANK:]
    n_part = swap(psend.at[oc], precv)
    phase("d2d_part")
    sends.landed(n_part, precv, partner)
    xb[0] = (psend[c] + precv[...]).astype(BF)

    sent_z = sends.sent_group(xb.at[pl.ds(0, ZN - 1)])
    nz = {o % ZN: sends.received_group() for o, _ in Z_RELAY}
    rest_z = sends.received_group()

    def z_send(o, d):
        sends.start(
            sent_z,
            nz.get((o + d) % ZN, rest_z),
            xb.at[o % ZN],
            xb.at[(o + d) % ZN],
            (y, x, wrap(z + d, ZN), c),
        )

    def z_landed(o):
        sends.landed(nz[o % ZN], xb.at[o % ZN], partner)

    phase("z_send")
    for d in Z_FIRST:
        z_send(0, d)
    n_basis = swap(basis.at[:, c], basis.at[:, c])
    next(gather_masters)
    phase("z_relay1")
    for o, hops in Z_RELAY[:2]:
        z_landed(o)
        for d in hops:
            z_send(o, d)
    phase("z_relay2")
    for o, hops in Z_RELAY[2:]:
        z_landed(o)
        for d in hops:
            z_send(o, d)
    phase("masters")
    next(gather_masters)
    next(gather_masters)
    next(gather_masters)
    phase("z_rest")
    sends.landed(rest_z, xb.at[pl.ds(0, ZN - 1 - len(nz))], partner)
    sends.landed(n_basis, basis.at[:, oc], partner)

    phase("low")
    low_t = jnp.dot(cot_t[...], xb[...].reshape(TOK, RANK), preferred_element_type=F32)
    lowf[...] = low_t.T.reshape(FN, LOW, 2 * HD)
    lowp[...] = lowf[...].astype(BF)
    all_low = lowr.at[pl.ds(1, FN - 1)]
    sent_low, got_low = sends.sent_group(all_low), sends.received_group()
    for dy, dx in PLANE:
        ty, tx = wrap(y + dy, YN), wrap(x + dx, XN)
        sends.start(sent_low, got_low, lowp.at[ty * XN + tx], lowr.at[dy * XN + dx], (ty, tx, z, c))
    phase("low_m")
    next(gather_masters)
    phase("low_recv")
    low = lowf[f]
    sends.landed(got_low, all_low, partner)
    for k in range(1, FN):
        low = low + lowr[k].astype(F32)

    phase("moments")
    all_ratios = xs.at[pl.ds(0, (2 * FN - 1) * LOW)]
    sent_r, got_r = sends.sent_group(all_ratios), sends.received_group()
    for k, (first, second) in enumerate(
        ((mom[c, 0], mom[c, 1]), (mom_other[0], mom_other[1]))
    ):
        part = low[:, k * HD : (k + 1) * HD]
        first_new = moment_decay * first + (1.0 - moment_decay) * part
        second_new = square_decay * second + (1.0 - square_decay) * part * part
        rsend[k] = (first_new / jnp.sqrt(second_new + square_floor)).astype(BF)
        if k == 0:
            moments_out[c, 0] = first_new
            moments_out[c, 1] = second_new
        else:
            msend[0] = first_new
            msend[1] = second_new
    ratios[c, f] = rsend[0]
    for dy, dx in PLANE + [(0, 0)]:
        ty, tx = wrap(y + dy, YN), wrap(x + dx, XN)
        for k, core in ((0, c), (1, oc)):
            if k == 0 and (dy, dx) == (0, 0):
                continue
            sends.start(sent_r, got_r, rsend.at[k], ratios.at[c, f], (ty, tx, z, core))
    n_out = swap(msend, moments_out.at[c])
    phase("masters_rest")
    for _ in gather_masters:
        pass
    phase("ratio_recv")
    sends.landed(got_r, all_ratios, partner)
    phase("fin")
    sends.landed(n_out, moments_out.at[oc], partner)
    sends.finish(partner)
    assert sends.sent <= N_SENT and sends.received <= N_RECEIVED
    phase(None)


N_SENT, N_RECEIVED = 11, 43


GROUP = 4
GROUPS = FN // GROUP


def finish(
    basis, masters, ratios, moments, own,
    q_step, q_weight, q_copy, q_first, q_second,
    k_step, k_weight, k_copy, k_first, k_second,
    held, steps, weights, copies,
    store_sem,
):
    f = lax.axis_index("y") * XN + lax.axis_index("x")
    stores = []
    phase = Phases()

    def store(src, dst):
        copy = pltpu.make_async_copy(src, dst, store_sem.at[len(stores)])
        copy.start()
        stores.append(copy)

    phase("product")
    ratio = [ratios[m].reshape(RANK, HD) for m in range(2)]
    totals = [jnp.zeros((8, HD), F32) for _ in range(2)]
    for g in range(GROUPS):
        for k in range(g * GROUP, (g + 1) * GROUP):
            for m in range(2):
                rows = basis[k, :, :, m * RANK : (m + 1) * RANK].reshape(ROWS, RANK)
                update = jnp.dot(rows, ratio[m], preferred_element_type=F32)
                held[m, k] = update
                totals[m] += jnp.sum((update * update).reshape(ROWS // 8, 8, HD), axis=0)
    phase("scale")
    for m, refs in enumerate(((q_first, q_second), (k_first, k_second))):
        for i in range(2):
            store(moments.at[m, i], refs[i])
    scales = [1.0 / jnp.sqrt(jnp.sum(t) / (D * HD) + norm_floor) for t in totals]
    for m, (step_ref, weight_ref) in enumerate(((q_step, q_weight), (k_step, k_weight))):
        step = held[m, f] * scales[m]
        steps[m] = step
        weights[m] = own[m] - step_rate * step
        store(steps.at[m], step_ref)
        store(weights.at[m], weight_ref)
    phase("copies")
    for g in range(GROUPS):
        for m, copy_ref in enumerate((q_copy, k_copy)):
            for k in range(g * GROUP, (g + 1) * GROUP):
                old = masters[k, :, m * HD : (m + 1) * HD].astype(F32)
                copies[m, k * ROWS : (k + 1) * ROWS] = (
                    old - step_rate * (held[m, k] * scales[m])
                ).astype(BF)
            rows = pl.ds(g * GROUP * ROWS, GROUP * ROWS)
            store(copies.at[m, rows], copy_ref.at[rows])
    phase("drain")
    for copy in stores:
        copy.wait()
    phase(None)


def body(*args):
    hbm = pl.BlockSpec(memory_space=pltpu.HBM)
    vmem = pl.BlockSpec(memory_space=pltpu.VMEM)
    dma = pltpu.SemaphoreType.DMA
    handed = pl.pallas_call(
        exchange,
        name="exchange",
        out_shape=(
            jax.ShapeDtypeStruct((FN, CN, HALF, 2 * RANK), BF),
            jax.ShapeDtypeStruct((FN, ROWS, 2 * HD), BF),
            jax.ShapeDtypeStruct((2, FN, LOW, HD), BF),
            jax.ShapeDtypeStruct((2, 2, LOW, HD), F32),
            jax.ShapeDtypeStruct((2, ROWS, HD), F32),
        ),
        in_specs=[hbm] * len(args),
        out_specs=(vmem,) * 5,
        scratch_shapes=[
            pltpu.VMEM((TOK, HD), BF),
            pltpu.VMEM((SUB, ZN * HD), BF),
            pltpu.VMEM((2, TOK, HD), BF),
            pltpu.VMEM((TOK, HD), BF),
            pltpu.VMEM((TOK, 2 * HD), BF),
            pltpu.VMEM((2 * HD, TOK), BF),
            pltpu.VMEM((2, 2, LOW, HD), F32),
            pltpu.VMEM((2, LOW, HD), F32),
            pltpu.VMEM((2, SUB, RANK), F32),
            pltpu.VMEM((SUB, RANK), F32),
            pltpu.VMEM((ZN, SUB, RANK), BF),
            pltpu.VMEM((FN, LOW, 2 * HD), F32),
            pltpu.VMEM((FN, LOW, 2 * HD), BF),
            pltpu.VMEM((FN, LOW, 2 * HD), BF),
            pltpu.VMEM((2, LOW, HD), BF),
            pltpu.VMEM((2, LOW, HD), F32),
            dma((11,)),
            dma((N_SENT,)),
            dma((N_RECEIVED,)),
        ],
        compiler_params=pltpu.CompilerParams(
            collective_id=0, has_side_effects=True, vmem_limit_bytes=VMEM_GRANT
        ),
    )(*(pltpu.with_memory_space_constraint(a, pltpu.HBM) for a in args))
    matrix = jax.ShapeDtypeStruct((ROWS, HD), F32)
    whole = jax.ShapeDtypeStruct((D, HD), BF)
    moment = jax.ShapeDtypeStruct((LOW, HD), F32)
    return pl.pallas_call(
        finish,
        name="finish",
        out_shape=(matrix, matrix, whole, moment, moment) * 2,
        in_specs=[vmem] * 5,
        out_specs=(hbm,) * 10,
        scratch_shapes=[
            pltpu.VMEM((2, FN, ROWS, HD), F32),
            pltpu.VMEM((2, ROWS, HD), F32),
            pltpu.VMEM((2, ROWS, HD), F32),
            pltpu.VMEM((2, D, HD), BF),
            dma((8 + 2 * GROUPS,)),
        ],
        compiler_params=pltpu.CompilerParams(vmem_limit_bytes=VMEM_GRANT),
    )(*handed)


def solution(mesh):
    torus = Mesh(mesh.devices.reshape(YN, XN, ZN, CN), AXES)
    split = P(FS, TP)
    in_specs = (split,) * 5 + (P(FS, None),) * 2 + (split,) * 4
    out_specs = (split, split, P(None, TP), split, split) * 2
    return jax.shard_map(body, mesh=torus, in_specs=in_specs, out_specs=out_specs, check_vma=False)
```

```python
import jax
import jax.numpy as jnp
from jax import lax
from jax.experimental import pallas as pl
from jax.experimental.pallas import tpu as pltpu
from jax.sharding import Mesh
from jax.sharding import PartitionSpec as P

D = 4096
HD = 128
RANK = 256
YN, XN, ZN, CN = 4, 4, 16, 2
FN = YN * XN
TOK = 1024
SUB = TOK // ZN
ROWS = D // FN
HALF = ROWS // CN
LOW = RANK // FN
CUTS = 2
CUT = SUB // CUTS
AXES = ("y", "x", "z", "c")
FS = ("y", "x")
TP = ("z", "c")

moment_decay = 0.8
square_decay = 0.9
square_floor = 1.0
norm_floor = 0.01
step_rate = 0.01

VMEM_GRANT = 20 * 1024 * 1024
MESH_ID = pl.DeviceIdType.MESH
BF = jnp.bfloat16
F32 = jnp.float32

PLANE = sorted(
    [(dy, dx) for dy in range(YN) for dx in range(XN) if (dy, dx) != (0, 0)],
    key=lambda o: -(min(o[0], 4 - o[0]) + min(o[1], 4 - o[1])),
)
ALONG_Z = [8, 7, -7, 6, -6, 5, -5, 4, -4, 3, -3, 2, -2, 1, -1]
Z_FIRST = [5, -5, 2, -2, 1, -1]
Z_RELAY = [(5, (3, 2, 1, -1)), (-5, (-2, -1, 1)), (2, (1,)), (-2, (-1,))]


class Phases:
    def __init__(self):
        self.open = None

    def __call__(self, name):
        if self.open is not None:
            self.open.__exit__(None, None, None)
        self.open = jax.named_scope(name) if name else None
        if self.open is not None:
            self.open.__enter__()


class Sends:
    def __init__(self, send_sem, recv_sem):
        self.send_sem, self.recv_sem = send_sem, recv_sem
        self.sent = self.received = 0
        self.open = []

    def sent_group(self, whole):
        self.open.append((self.sent, whole))
        self.sent += 1
        return self.sent - 1

    def received_group(self):
        self.received += 1
        return self.received - 1

    def start(self, sent, received, src, dst, device):
        pltpu.make_async_remote_copy(
            src_ref=src,
            dst_ref=dst,
            send_sem=self.send_sem.at[sent],
            recv_sem=self.recv_sem.at[received],
            device_id=device,
            device_id_type=MESH_ID,
        ).start()

    def whole(self, sent, received, ref, device):
        return pltpu.make_async_remote_copy(
            src_ref=ref,
            dst_ref=ref,
            send_sem=self.send_sem.at[sent],
            recv_sem=self.recv_sem.at[received],
            device_id=device,
            device_id_type=MESH_ID,
        )

    def landed(self, received, ref, device):
        self.whole(0, received, ref, device).wait_recv()

    def finish(self, device):
        for group, ref in self.open:
            self.whole(group, 0, ref, device).wait_send()


def wrap(value, count):
    return lax.rem(value + 2 * count, count)


def plane_gather(sends, piece, many, me, rows):
    y, x, z, c = me
    half, quarter = rows // 2, rows // 4
    signs = (1, -1)

    def shift(h, first, second):
        d1, d2 = (first, second)
        dy, dx = (d2, d1) if h == 0 else (d1, d2)
        return wrap(y + dy, YN), wrap(x + dx, XN)

    def ref(h, first, second, part=None):
        fy, fx = shift(h, first, second)
        start = h * half + (0 if part is None else part * quarter)
        return piece(fy, fx, start, half if part is None else quarter)

    def dev(h, first, second):
        fy, fx = shift(h, first, second)
        return (fy, fx, z, c)

    part_of = {1: 0, -1: 1}
    halves = (0, 1)
    sent = sends.sent_group(many(FN - 1, 0, rows))
    n1 = {h: sends.received_group() for h in halves}
    n1r = {h: sends.received_group() for h in halves}
    n2 = {(h, j): sends.received_group() for j in (0, -1, 1, 2) for h in halves}
    n2r = sends.received_group()
    me_dev = dev(0, 1, 0)

    def go(number, source, target):
        sends.start(sent, number, source, source, target)

    def second_stage(h, j):
        for s in signs:
            go(n2[h, j], ref(h, j, 0), dev(h, 0, s))

    def second_relay(h, j):
        sends.landed(n2[h, j], many(2, 0, half), me_dev)
        for s in signs:
            go(n2r, ref(h, j, -s, part_of[s]), dev(h, 0, s))

    for h in halves:
        for s in signs:
            go(n1[h], ref(h, 0, 0), dev(h, s, 0))
    for h in halves:
        second_stage(h, 0)
    yield
    for h in halves:
        sends.landed(n1[h], many(2, 0, half), me_dev)
        for s in signs:
            go(n1r[h], ref(h, -s, 0, part_of[s]), dev(h, s, 0))
    for h in halves:
        second_stage(h, -1)
        second_stage(h, 1)
    yield
    for h in halves:
        second_relay(h, 0)
    yield
    for h in halves:
        sends.landed(n1r[h], many(1, 0, half), me_dev)
        second_stage(h, 2)
    yield
    for j in (-1, 1):
        for h in halves:
            second_relay(h, j)
    yield
    for h in halves:
        second_relay(h, 2)
    yield
    sends.landed(n2r, many(8, 0, half), me_dev)


def exchange(
    x_in, qc_in, kc_in, qm_in, km_in, qb_in, kb_in, qf_in, qs_in, kf_in, ks_in,
    basis, masters, ratios, moments_out, mas,
    xs, xg, cots, cot_other, cot_rel, cot_t, mom, mom_other,
    psend, precv, xb, lowf, lowp, lowr, rsend, msend,
    load_sem, send_sem, recv_sem,
):
    y, x, z, c = (lax.axis_index(a) for a in AXES)
    me = (y, x, z, c)
    oc = 1 - c
    phase = Phases()
    f = y * XN + x
    partner = (y, x, z, oc)

    phase("enter")
    barrier = pltpu.get_barrier_semaphore()
    near = [(y, x, wrap(z + d, ZN), c) for d in ALONG_Z]
    near += [(wrap(y + dy, YN), wrap(x + dx, XN), z, core) for dy, dx in PLANE for core in (c, oc)]
    near += [partner]
    for device in near:
        pl.semaphore_signal(barrier, inc=1, device_id=device, device_id_type=MESH_ID)

    loads = []

    def load(src, dst):
        copy = pltpu.make_async_copy(src, dst, load_sem.at[len(loads)])
        copy.start()
        loads.append(copy)

    mine = pl.ds(pl.multiple_of(c * HALF, HALF), HALF)
    load(x_in, xs)
    load(qb_in.at[mine], basis.at[f, c, :, pl.ds(0, RANK)])
    load(kb_in.at[mine], basis.at[f, c, :, pl.ds(RANK, RANK)])
    load(qc_in, cots.at[0])
    load(kc_in, cots.at[1])
    load(qf_in, mom.at[0, 0])
    load(qs_in, mom.at[0, 1])
    load(kf_in, mom.at[1, 0])
    load(ks_in, mom.at[1, 1])
    load(qm_in, mas.at[0])
    load(km_in, mas.at[1])
    phase("loads")
    for copy in loads[:3]:
        copy.wait()
    sends = Sends(send_sem, recv_sem)
    phase("barrier")
    pl.semaphore_wait(barrier, len(near))

    phase("send_inputs")
    def xslot(zz):
        return xg.at[:, pl.ds(pl.multiple_of(zz * HD, HD), HD)]

    several = xs.at[pl.ds(0, (ZN - 1) * SUB)]
    sent_x, got_x = sends.sent_group(several), sends.received_group()
    gather_basis = plane_gather(
        sends,
        lambda fy, fx, s, n: basis.at[fy * XN + fx, c, pl.ds(s, n)],
        lambda k, s, n: basis.at[pl.ds(0, k), 0, pl.ds(s, n)],
        me,
        HALF,
    )
    gather_masters = plane_gather(
        sends,
        lambda fy, fx, s, n: masters.at[fy * XN + fx, pl.ds(s, n)],
        lambda k, s, n: masters.at[pl.ds(0, k), pl.ds(s, n)],
        me,
        ROWS,
    )
    next(gather_basis)
    for d in ALONG_Z:
        zz = wrap(z + d, ZN)
        rows = xs.at[pl.ds(pl.multiple_of(zz * SUB, SUB), SUB)]
        sends.start(sent_x, got_x, rows, xslot(z), (y, x, zz, c))
    for copy in loads[3:]:
        copy.wait()

    def swap(src, dst):
        received = sends.received_group()
        sends.start(sends.sent_group(src), received, src, dst, partner)
        return received

    n_cot = swap(cots.at[oc], cot_other)
    n_mom = swap(mom.at[oc], mom_other)
    xg[:, pl.ds(pl.multiple_of(z * HD, HD), HD)] = xs[pl.ds(pl.multiple_of(z * SUB, SUB), SUB), :]
    masters[f, :, 0:HD] = mas[0].astype(BF)
    masters[f, :, HD : 2 * HD] = mas[1].astype(BF)
    phase("basis_1")
    next(gather_basis)

    phase("cot_rel")
    sends.landed(n_cot, cot_other, partner)
    sends.landed(n_mom, mom_other, partner)
    for o in range(ZN):
        zz = wrap(z - o, ZN)
        rows = pl.ds(pl.multiple_of(zz * SUB, SUB), SUB)
        cot_rel[o * SUB : (o + 1) * SUB, 0:HD] = cots[c, rows, :]
        cot_rel[o * SUB : (o + 1) * SUB, HD : 2 * HD] = cot_other[rows, :]
    phase("basis_23")
    next(gather_basis)
    next(gather_basis)
    phase("cot_t")
    cot_t[...] = cot_rel[...].T
    phase("basis_rest")
    for _ in gather_basis:
        pass
    phase("wait_x")
    sends.landed(got_x, several, partner)

    phase("xb")
    part = jnp.zeros((SUB, 2 * RANK), F32)
    for k in range(FN // 2):
        rows = basis[2 * k : 2 * k + 2, c].reshape(2 * HALF, 2 * RANK)
        part += jnp.dot(
            xg[:, k * 2 * HD : (k + 1) * 2 * HD], rows, preferred_element_type=F32
        )
    psend[0] = part[:, :RANK]
    psend[1] = part[:, RANK:]
    n_part = swap(psend.at[oc], precv)
    phase("d2d_part")
    sends.landed(n_part, precv, partner)
    xb[0] = (psend[c] + precv[...]).astype(BF)

    sent_z = sends.sent_group(xb.at[pl.ds(0, ZN - 1)])
    nz = {(o % ZN, k): sends.received_group() for o, _ in Z_RELAY for k in range(CUTS)}
    rest_z = sends.received_group()

    def z_send(o, d, k):
        rows = pl.ds(k * CUT, CUT)
        sends.start(
            sent_z,
            nz.get(((o + d) % ZN, k), rest_z),
            xb.at[o % ZN, rows],
            xb.at[(o + d) % ZN, rows],
            (y, x, wrap(z + d, ZN), c),
        )

    phase("z_send")
    for d in Z_FIRST:
        for k in range(CUTS):
            z_send(0, d, k)
    n_basis = swap(basis.at[:, c], basis.at[:, c])
    next(gather_masters)
    next(gather_masters)
    phase("z_relay1")
    for k in range(CUTS):
        for o, hops in Z_RELAY:
            sends.landed(nz[o % ZN, k], xb.at[o % ZN, pl.ds(k * CUT, CUT)], partner)
            for d in hops:
                z_send(o, d, k)
    phase("masters")
    next(gather_masters)
    next(gather_masters)
    next(gather_masters)
    phase("z_rest")
    sends.landed(rest_z, xb.at[pl.ds(0, ZN - 1 - len(Z_RELAY))], partner)
    sends.landed(n_basis, basis.at[:, oc], partner)

    phase("low")
    low_t = jnp.dot(cot_t[...], xb[...].reshape(TOK, RANK), preferred_element_type=F32)
    lowf[...] = low_t.T.reshape(FN, LOW, 2 * HD)
    lowp[...] = lowf[...].astype(BF)
    all_low = lowr.at[pl.ds(1, FN - 1)]
    sent_low, got_low = sends.sent_group(all_low), sends.received_group()
    for dy, dx in PLANE:
        ty, tx = wrap(y + dy, YN), wrap(x + dx, XN)
        sends.start(sent_low, got_low, lowp.at[ty * XN + tx], lowr.at[dy * XN + dx], (ty, tx, z, c))
    phase("low_m")
    next(gather_masters)
    phase("low_recv")
    low = lowf[f]
    sends.landed(got_low, all_low, partner)
    for k in range(1, FN):
        low = low + lowr[k].astype(F32)

    phase("moments")
    all_ratios = xs.at[pl.ds(0, (2 * FN - 1) * LOW)]
    sent_r, got_r = sends.sent_group(all_ratios), sends.received_group()
    for k, (first, second) in enumerate(
        ((mom[c, 0], mom[c, 1]), (mom_other[0], mom_other[1]))
    ):
        part = low[:, k * HD : (k + 1) * HD]
        first_new = moment_decay * first + (1.0 - moment_decay) * part
        second_new = square_decay * second + (1.0 - square_decay) * part * part
        rsend[k] = (first_new / jnp.sqrt(second_new + square_floor)).astype(BF)
        if k == 0:
            moments_out[c, 0] = first_new
            moments_out[c, 1] = second_new
        else:
            msend[0] = first_new
            msend[1] = second_new
    ratios[c, f] = rsend[0]
    for dy, dx in PLANE + [(0, 0)]:
        ty, tx = wrap(y + dy, YN), wrap(x + dx, XN)
        for k, core in ((0, c), (1, oc)):
            if k == 0 and (dy, dx) == (0, 0):
                continue
            sends.start(sent_r, got_r, rsend.at[k], ratios.at[c, f], (ty, tx, z, core))
    n_out = swap(msend, moments_out.at[c])
    phase("masters_rest")
    for _ in gather_masters:
        pass
    phase("ratio_recv")
    sends.landed(got_r, all_ratios, partner)
    phase("fin")
    sends.landed(n_out, moments_out.at[oc], partner)
    sends.finish(partner)
    assert sends.sent <= N_SENT and sends.received <= N_RECEIVED
    phase(None)


N_SENT, N_RECEIVED = 11, 43 + 4 * (CUTS - 1)


GROUP = 4
GROUPS = FN // GROUP


def finish(
    basis, masters, ratios, moments, own,
    q_step, q_weight, q_copy, q_first, q_second,
    k_step, k_weight, k_copy, k_first, k_second,
    held, steps, weights, copies,
    store_sem,
):
    f = lax.axis_index("y") * XN + lax.axis_index("x")
    stores = []
    phase = Phases()

    def store(src, dst):
        copy = pltpu.make_async_copy(src, dst, store_sem.at[len(stores)])
        copy.start()
        stores.append(copy)

    phase("product")
    ratio = [ratios[m].reshape(RANK, HD) for m in range(2)]
    totals = [jnp.zeros((8, HD), F32) for _ in range(2)]
    for g in range(GROUPS):
        for k in range(g * GROUP, (g + 1) * GROUP):
            for m in range(2):
                rows = basis[k, :, :, m * RANK : (m + 1) * RANK].reshape(ROWS, RANK)
                update = jnp.dot(rows, ratio[m], preferred_element_type=F32)
                held[m, k] = update
                totals[m] += jnp.sum((update * update).reshape(ROWS // 8, 8, HD), axis=0)
    phase("scale")
    for m, refs in enumerate(((q_first, q_second), (k_first, k_second))):
        for i in range(2):
            store(moments.at[m, i], refs[i])
    scales = [1.0 / jnp.sqrt(jnp.sum(t) / (D * HD) + norm_floor) for t in totals]
    for m, (step_ref, weight_ref) in enumerate(((q_step, q_weight), (k_step, k_weight))):
        step = held[m, f] * scales[m]
        steps[m] = step
        weights[m] = own[m] - step_rate * step
        store(steps.at[m], step_ref)
        store(weights.at[m], weight_ref)
    phase("copies")
    for g in range(GROUPS):
        for m, copy_ref in enumerate((q_copy, k_copy)):
            for k in range(g * GROUP, (g + 1) * GROUP):
                old = masters[k, :, m * HD : (m + 1) * HD].astype(F32)
                copies[m, k * ROWS : (k + 1) * ROWS] = (
                    old - step_rate * (held[m, k] * scales[m])
                ).astype(BF)
            rows = pl.ds(g * GROUP * ROWS, GROUP * ROWS)
            store(copies.at[m, rows], copy_ref.at[rows])
    phase("drain")
    for copy in stores:
        copy.wait()
    phase(None)


def body(*args):
    hbm = pl.BlockSpec(memory_space=pltpu.HBM)
    vmem = pl.BlockSpec(memory_space=pltpu.VMEM)
    dma = pltpu.SemaphoreType.DMA
    handed = pl.pallas_call(
        exchange,
        name="exchange",
        out_shape=(
            jax.ShapeDtypeStruct((FN, CN, HALF, 2 * RANK), BF),
            jax.ShapeDtypeStruct((FN, ROWS, 2 * HD), BF),
            jax.ShapeDtypeStruct((2, FN, LOW, HD), BF),
            jax.ShapeDtypeStruct((2, 2, LOW, HD), F32),
            jax.ShapeDtypeStruct((2, ROWS, HD), F32),
        ),
        in_specs=[hbm] * len(args),
        out_specs=(vmem,) * 5,
        scratch_shapes=[
            pltpu.VMEM((TOK, HD), BF),
            pltpu.VMEM((SUB, ZN * HD), BF),
            pltpu.VMEM((2, TOK, HD), BF),
            pltpu.VMEM((TOK, HD), BF),
            pltpu.VMEM((TOK, 2 * HD), BF),
            pltpu.VMEM((2 * HD, TOK), BF),
            pltpu.VMEM((2, 2, LOW, HD), F32),
            pltpu.VMEM((2, LOW, HD), F32),
            pltpu.VMEM((2, SUB, RANK), F32),
            pltpu.VMEM((SUB, RANK), F32),
            pltpu.VMEM((ZN, SUB, RANK), BF),
            pltpu.VMEM((FN, LOW, 2 * HD), F32),
            pltpu.VMEM((FN, LOW, 2 * HD), BF),
            pltpu.VMEM((FN, LOW, 2 * HD), BF),
            pltpu.VMEM((2, LOW, HD), BF),
            pltpu.VMEM((2, LOW, HD), F32),
            dma((11,)),
            dma((N_SENT,)),
            dma((N_RECEIVED,)),
        ],
        compiler_params=pltpu.CompilerParams(
            collective_id=0, has_side_effects=True, vmem_limit_bytes=VMEM_GRANT
        ),
    )(*(pltpu.with_memory_space_constraint(a, pltpu.HBM) for a in args))
    matrix = jax.ShapeDtypeStruct((ROWS, HD), F32)
    whole = jax.ShapeDtypeStruct((D, HD), BF)
    moment = jax.ShapeDtypeStruct((LOW, HD), F32)
    return pl.pallas_call(
        finish,
        name="finish",
        out_shape=(matrix, matrix, whole, moment, moment) * 2,
        in_specs=[vmem] * 5,
        out_specs=(hbm,) * 10,
        scratch_shapes=[
            pltpu.VMEM((2, FN, ROWS, HD), F32),
            pltpu.VMEM((2, ROWS, HD), F32),
            pltpu.VMEM((2, ROWS, HD), F32),
            pltpu.VMEM((2, D, HD), BF),
            dma((8 + 2 * GROUPS,)),
        ],
        compiler_params=pltpu.CompilerParams(vmem_limit_bytes=VMEM_GRANT),
    )(*handed)


def solution(mesh):
    torus = Mesh(mesh.devices.reshape(YN, XN, ZN, CN), AXES)
    split = P(FS, TP)
    in_specs = (split,) * 5 + (P(FS, None),) * 2 + (split,) * 4
    out_specs = (split, split, P(None, TP), split, split) * 2
    return jax.shard_map(body, mesh=torus, in_specs=in_specs, out_specs=out_specs, check_vma=False)
```

```python
import jax
import jax.numpy as jnp
from jax import lax
from jax.experimental import pallas as pl
from jax.experimental.pallas import tpu as pltpu
from jax.sharding import Mesh
from jax.sharding import PartitionSpec as P

D = 4096
HD = 128
RANK = 256
YN, XN, ZN, CN = 4, 4, 16, 2
FN = YN * XN
TOK = 1024
SUB = TOK // ZN
ROWS = D // FN
HALF = ROWS // CN
LOW = RANK // FN
CUTS = 2
CUT = SUB // CUTS
AXES = ("y", "x", "z", "c")
FS = ("y", "x")
TP = ("z", "c")

moment_decay = 0.8
square_decay = 0.9
square_floor = 1.0
norm_floor = 0.01
step_rate = 0.01

VMEM_GRANT = 20 * 1024 * 1024
MESH_ID = pl.DeviceIdType.MESH
BF = jnp.bfloat16
F32 = jnp.float32

PLANE = sorted(
    [(dy, dx) for dy in range(YN) for dx in range(XN) if (dy, dx) != (0, 0)],
    key=lambda o: -(min(o[0], 4 - o[0]) + min(o[1], 4 - o[1])),
)
ALONG_Z = [8, 7, -7, 6, -6, 5, -5, 4, -4, 3, -3, 2, -2, 1, -1]
Z_FIRST = [5, -5, 2, -2, 1, -1]
Z_RELAY = [
    [(5, (3, 2, 1, -1)), (-5, (-2, -1, 1)), (2, (1,)), (-2, (-1,))],
    [(5, (2, 1, -1)), (-5, (-3, -2, -1, 1)), (2, (1,)), (-2, (-1,))],
]


class Phases:
    def __init__(self):
        self.open = None

    def __call__(self, name):
        if self.open is not None:
            self.open.__exit__(None, None, None)
        self.open = jax.named_scope(name) if name else None
        if self.open is not None:
            self.open.__enter__()


class Sends:
    def __init__(self, send_sem, recv_sem):
        self.send_sem, self.recv_sem = send_sem, recv_sem
        self.sent = self.received = 0
        self.open = []

    def sent_group(self, whole):
        self.open.append((self.sent, whole))
        self.sent += 1
        return self.sent - 1

    def received_group(self):
        self.received += 1
        return self.received - 1

    def start(self, sent, received, src, dst, device):
        pltpu.make_async_remote_copy(
            src_ref=src,
            dst_ref=dst,
            send_sem=self.send_sem.at[sent],
            recv_sem=self.recv_sem.at[received],
            device_id=device,
            device_id_type=MESH_ID,
        ).start()

    def whole(self, sent, received, ref, device):
        return pltpu.make_async_remote_copy(
            src_ref=ref,
            dst_ref=ref,
            send_sem=self.send_sem.at[sent],
            recv_sem=self.recv_sem.at[received],
            device_id=device,
            device_id_type=MESH_ID,
        )

    def landed(self, received, ref, device):
        self.whole(0, received, ref, device).wait_recv()

    def finish(self, device):
        for group, ref in self.open:
            self.whole(group, 0, ref, device).wait_send()


def wrap(value, count):
    return lax.rem(value + 2 * count, count)


def plane_gather(sends, piece, many, me, rows):
    y, x, z, c = me
    half, quarter = rows // 2, rows // 4
    signs = (1, -1)

    def shift(h, first, second):
        d1, d2 = (first, second)
        dy, dx = (d2, d1) if h == 0 else (d1, d2)
        return wrap(y + dy, YN), wrap(x + dx, XN)

    def ref(h, first, second, part=None):
        fy, fx = shift(h, first, second)
        start = h * half + (0 if part is None else part * quarter)
        return piece(fy, fx, start, half if part is None else quarter)

    def dev(h, first, second):
        fy, fx = shift(h, first, second)
        return (fy, fx, z, c)

    part_of = {1: 0, -1: 1}
    halves = (0, 1)
    sent = sends.sent_group(many(FN - 1, 0, rows))
    n1 = {h: sends.received_group() for h in halves}
    n1r = {h: sends.received_group() for h in halves}
    n2 = {(h, j): sends.received_group() for j in (0, -1, 1, 2) for h in halves}
    n2r = sends.received_group()
    me_dev = dev(0, 1, 0)

    def go(number, source, target):
        sends.start(sent, number, source, source, target)

    def second_stage(h, j):
        for s in signs:
            go(n2[h, j], ref(h, j, 0), dev(h, 0, s))

    def second_relay(h, j):
        sends.landed(n2[h, j], many(2, 0, half), me_dev)
        for s in signs:
            go(n2r, ref(h, j, -s, part_of[s]), dev(h, 0, s))

    for h in halves:
        for s in signs:
            go(n1[h], ref(h, 0, 0), dev(h, s, 0))
    for h in halves:
        second_stage(h, 0)
    yield
    for h in halves:
        sends.landed(n1[h], many(2, 0, half), me_dev)
        for s in signs:
            go(n1r[h], ref(h, -s, 0, part_of[s]), dev(h, s, 0))
    for h in halves:
        second_stage(h, -1)
        second_stage(h, 1)
    yield
    for h in halves:
        second_relay(h, 0)
    yield
    for h in halves:
        sends.landed(n1r[h], many(1, 0, half), me_dev)
        second_stage(h, 2)
    yield
    for j in (-1, 1):
        for h in halves:
            second_relay(h, j)
    yield
    for h in halves:
        second_relay(h, 2)
    yield
    sends.landed(n2r, many(8, 0, half), me_dev)


def exchange(
    x_in, qc_in, kc_in, qm_in, km_in, qb_in, kb_in, qf_in, qs_in, kf_in, ks_in,
    basis, masters, ratios, moments_out, mas,
    xs, xg, cots, cot_other, cot_rel, cot_t, mom, mom_other,
    psend, precv, xb, lowf, lowp, lowr, rsend, msend,
    load_sem, send_sem, recv_sem,
):
    y, x, z, c = (lax.axis_index(a) for a in AXES)
    me = (y, x, z, c)
    oc = 1 - c
    phase = Phases()
    f = y * XN + x
    partner = (y, x, z, oc)

    phase("enter")
    barrier = pltpu.get_barrier_semaphore()
    near = [(y, x, wrap(z + d, ZN), c) for d in ALONG_Z]
    near += [(wrap(y + dy, YN), wrap(x + dx, XN), z, core) for dy, dx in PLANE for core in (c, oc)]
    near += [partner]
    for device in near:
        pl.semaphore_signal(barrier, inc=1, device_id=device, device_id_type=MESH_ID)

    loads = []

    def load(src, dst):
        copy = pltpu.make_async_copy(src, dst, load_sem.at[len(loads)])
        copy.start()
        loads.append(copy)

    mine = pl.ds(pl.multiple_of(c * HALF, HALF), HALF)
    load(x_in, xs)
    load(qb_in.at[mine], basis.at[f, c, :, pl.ds(0, RANK)])
    load(kb_in.at[mine], basis.at[f, c, :, pl.ds(RANK, RANK)])
    load(qc_in, cots.at[0])
    load(kc_in, cots.at[1])
    load(qf_in, mom.at[0, 0])
    load(qs_in, mom.at[0, 1])
    load(kf_in, mom.at[1, 0])
    load(ks_in, mom.at[1, 1])
    load(qm_in, mas.at[0])
    load(km_in, mas.at[1])
    phase("loads")
    for copy in loads[:3]:
        copy.wait()
    sends = Sends(send_sem, recv_sem)
    phase("barrier")
    pl.semaphore_wait(barrier, len(near))

    phase("send_inputs")
    def xslot(zz):
        return xg.at[:, pl.ds(pl.multiple_of(zz * HD, HD), HD)]

    several = xs.at[pl.ds(0, (ZN - 1) * SUB)]
    sent_x, got_x = sends.sent_group(several), sends.received_group()
    gather_basis = plane_gather(
        sends,
        lambda fy, fx, s, n: basis.at[fy * XN + fx, c, pl.ds(s, n)],
        lambda k, s, n: basis.at[pl.ds(0, k), 0, pl.ds(s, n)],
        me,
        HALF,
    )
    gather_masters = plane_gather(
        sends,
        lambda fy, fx, s, n: masters.at[fy * XN + fx, pl.ds(s, n)],
        lambda k, s, n: masters.at[pl.ds(0, k), pl.ds(s, n)],
        me,
        ROWS,
    )
    next(gather_basis)
    for d in ALONG_Z:
        zz = wrap(z + d, ZN)
        rows = xs.at[pl.ds(pl.multiple_of(zz * SUB, SUB), SUB)]
        sends.start(sent_x, got_x, rows, xslot(z), (y, x, zz, c))
    for copy in loads[3:]:
        copy.wait()

    def swap(src, dst):
        received = sends.received_group()
        sends.start(sends.sent_group(src), received, src, dst, partner)
        return received

    n_cot = swap(cots.at[oc], cot_other)
    n_mom = swap(mom.at[oc], mom_other)
    xg[:, pl.ds(pl.multiple_of(z * HD, HD), HD)] = xs[pl.ds(pl.multiple_of(z * SUB, SUB), SUB), :]
    masters[f, :, 0:HD] = mas[0].astype(BF)
    masters[f, :, HD : 2 * HD] = mas[1].astype(BF)
    phase("basis_1")
    next(gather_basis)

    phase("cot_rel")
    sends.landed(n_cot, cot_other, partner)
    sends.landed(n_mom, mom_other, partner)
    for o in range(ZN):
        zz = wrap(z - o, ZN)
        rows = pl.ds(pl.multiple_of(zz * SUB, SUB), SUB)
        cot_rel[o * SUB : (o + 1) * SUB, 0:HD] = cots[c, rows, :]
        cot_rel[o * SUB : (o + 1) * SUB, HD : 2 * HD] = cot_other[rows, :]
    phase("basis_23")
    next(gather_basis)
    next(gather_basis)
    phase("cot_t")
    cot_t[...] = cot_rel[...].T
    phase("basis_rest")
    for _ in gather_basis:
        pass
    phase("wait_x")
    sends.landed(got_x, several, partner)

    phase("xb")
    part = jnp.zeros((SUB, 2 * RANK), F32)
    for k in range(FN // 2):
        rows = basis[2 * k : 2 * k + 2, c].reshape(2 * HALF, 2 * RANK)
        part += jnp.dot(
            xg[:, k * 2 * HD : (k + 1) * 2 * HD], rows, preferred_element_type=F32
        )
    psend[0] = part[:, :RANK]
    psend[1] = part[:, RANK:]
    n_part = swap(psend.at[oc], precv)
    phase("d2d_part")
    sends.landed(n_part, precv, partner)
    xb[0] = (psend[c] + precv[...]).astype(BF)

    sent_z = sends.sent_group(xb.at[pl.ds(0, ZN - 1)])
    nz = {(o % ZN, k): sends.received_group() for k in range(CUTS) for o, _ in Z_RELAY[k]}
    rest_z = sends.received_group()

    def z_send(o, d, k):
        rows = pl.ds(k * CUT, CUT)
        sends.start(
            sent_z,
            nz.get(((o + d) % ZN, k), rest_z),
            xb.at[o % ZN, rows],
            xb.at[(o + d) % ZN, rows],
            (y, x, wrap(z + d, ZN), c),
        )

    phase("z_send")
    for d in Z_FIRST:
        for k in range(CUTS):
            z_send(0, d, k)
    n_basis = swap(basis.at[:, c], basis.at[:, c])
    next(gather_masters)
    next(gather_masters)
    phase("z_relay1")
    for k in range(CUTS):
        for o, hops in Z_RELAY[k]:
            sends.landed(nz[o % ZN, k], xb.at[o % ZN, pl.ds(k * CUT, CUT)], partner)
            for d in hops:
                z_send(o, d, k)
    phase("masters")
    next(gather_masters)
    next(gather_masters)
    next(gather_masters)
    phase("z_rest")
    sends.landed(rest_z, xb.at[pl.ds(0, ZN - 1 - len(Z_RELAY[0]))], partner)
    sends.landed(n_basis, basis.at[:, oc], partner)

    phase("low")
    low_t = jnp.dot(cot_t[...], xb[...].reshape(TOK, RANK), preferred_element_type=F32)
    lowf[...] = low_t.T.reshape(FN, LOW, 2 * HD)
    lowp[...] = lowf[...].astype(BF)
    all_low = lowr.at[pl.ds(1, FN - 1)]
    sent_low, got_low = sends.sent_group(all_low), sends.received_group()
    for dy, dx in PLANE:
        ty, tx = wrap(y + dy, YN), wrap(x + dx, XN)
        sends.start(sent_low, got_low, lowp.at[ty * XN + tx], lowr.at[dy * XN + dx], (ty, tx, z, c))
    phase("low_m")
    next(gather_masters)
    phase("low_recv")
    low = lowf[f]
    sends.landed(got_low, all_low, partner)
    for k in range(1, FN):
        low = low + lowr[k].astype(F32)

    phase("moments")
    all_ratios = xs.at[pl.ds(0, (2 * FN - 1) * LOW)]
    sent_r, got_r = sends.sent_group(all_ratios), sends.received_group()
    for k, (first, second) in enumerate(
        ((mom[c, 0], mom[c, 1]), (mom_other[0], mom_other[1]))
    ):
        part = low[:, k * HD : (k + 1) * HD]
        first_new = moment_decay * first + (1.0 - moment_decay) * part
        second_new = square_decay * second + (1.0 - square_decay) * part * part
        rsend[k] = (first_new / jnp.sqrt(second_new + square_floor)).astype(BF)
        if k == 0:
            moments_out[c, 0] = first_new
            moments_out[c, 1] = second_new
        else:
            msend[0] = first_new
            msend[1] = second_new
    ratios[c, f] = rsend[0]
    for dy, dx in PLANE + [(0, 0)]:
        ty, tx = wrap(y + dy, YN), wrap(x + dx, XN)
        for k, core in ((0, c), (1, oc)):
            if k == 0 and (dy, dx) == (0, 0):
                continue
            sends.start(sent_r, got_r, rsend.at[k], ratios.at[c, f], (ty, tx, z, core))
    n_out = swap(msend, moments_out.at[c])
    phase("masters_rest")
    for _ in gather_masters:
        pass
    phase("ratio_recv")
    sends.landed(got_r, all_ratios, partner)
    phase("fin")
    sends.landed(n_out, moments_out.at[oc], partner)
    sends.finish(partner)
    assert sends.sent <= N_SENT and sends.received <= N_RECEIVED
    phase(None)


N_SENT, N_RECEIVED = 11, 43 + 4 * (CUTS - 1)


GROUP = 4
GROUPS = FN // GROUP


def finish(
    basis, masters, ratios, moments, own,
    q_step, q_weight, q_copy, q_first, q_second,
    k_step, k_weight, k_copy, k_first, k_second,
    held, steps, weights, copies,
    store_sem,
):
    f = lax.axis_index("y") * XN + lax.axis_index("x")
    stores = []
    phase = Phases()

    def store(src, dst):
        copy = pltpu.make_async_copy(src, dst, store_sem.at[len(stores)])
        copy.start()
        stores.append(copy)

    outs = (
        (q_step, q_weight, q_copy, q_first, q_second),
        (k_step, k_weight, k_copy, k_first, k_second),
    )
    for m, (step_ref, weight_ref, copy_ref, first_ref, second_ref) in enumerate(outs):
        store(moments.at[m, 0], first_ref)
        store(moments.at[m, 1], second_ref)
    for m, (step_ref, weight_ref, copy_ref, first_ref, second_ref) in enumerate(outs):
        phase(f"product_{m}")
        ratio = ratios[m].reshape(RANK, HD)
        total = jnp.zeros((8, HD), F32)
        for g in range(GROUPS):
            blocks = slice(g * GROUP, (g + 1) * GROUP)
            rows = basis[blocks, :, :, m * RANK : (m + 1) * RANK].reshape(GROUP * ROWS, RANK)
            update = jnp.dot(rows, ratio, preferred_element_type=F32)
            held[m, blocks] = update.reshape(GROUP, ROWS, HD)
            total += jnp.sum((update * update).reshape(GROUP * ROWS // 8, 8, HD), axis=0)
        phase(f"copies_{m}")
        scale = 1.0 / jnp.sqrt(jnp.sum(total) / (D * HD) + norm_floor)
        step = held[m, f] * scale
        steps[m] = step
        weights[m] = own[m] - step_rate * step
        store(steps.at[m], step_ref)
        store(weights.at[m], weight_ref)
        for g in range(GROUPS):
            for k in range(g * GROUP, (g + 1) * GROUP):
                old = masters[k, :, m * HD : (m + 1) * HD].astype(F32)
                copies[m, k * ROWS : (k + 1) * ROWS] = (
                    old - step_rate * (held[m, k] * scale)
                ).astype(BF)
            rows = pl.ds(g * GROUP * ROWS, GROUP * ROWS)
            store(copies.at[m, rows], copy_ref.at[rows])
    phase("drain")
    for copy in stores:
        copy.wait()
    phase(None)


def body(*args):
    hbm = pl.BlockSpec(memory_space=pltpu.HBM)
    vmem = pl.BlockSpec(memory_space=pltpu.VMEM)
    dma = pltpu.SemaphoreType.DMA
    handed = pl.pallas_call(
        exchange,
        name="exchange",
        out_shape=(
            jax.ShapeDtypeStruct((FN, CN, HALF, 2 * RANK), BF),
            jax.ShapeDtypeStruct((FN, ROWS, 2 * HD), BF),
            jax.ShapeDtypeStruct((2, FN, LOW, HD), BF),
            jax.ShapeDtypeStruct((2, 2, LOW, HD), F32),
            jax.ShapeDtypeStruct((2, ROWS, HD), F32),
        ),
        in_specs=[hbm] * len(args),
        out_specs=(vmem,) * 5,
        scratch_shapes=[
            pltpu.VMEM((TOK, HD), BF),
            pltpu.VMEM((SUB, ZN * HD), BF),
            pltpu.VMEM((2, TOK, HD), BF),
            pltpu.VMEM((TOK, HD), BF),
            pltpu.VMEM((TOK, 2 * HD), BF),
            pltpu.VMEM((2 * HD, TOK), BF),
            pltpu.VMEM((2, 2, LOW, HD), F32),
            pltpu.VMEM((2, LOW, HD), F32),
            pltpu.VMEM((2, SUB, RANK), F32),
            pltpu.VMEM((SUB, RANK), F32),
            pltpu.VMEM((ZN, SUB, RANK), BF),
            pltpu.VMEM((FN, LOW, 2 * HD), F32),
            pltpu.VMEM((FN, LOW, 2 * HD), BF),
            pltpu.VMEM((FN, LOW, 2 * HD), BF),
            pltpu.VMEM((2, LOW, HD), BF),
            pltpu.VMEM((2, LOW, HD), F32),
            dma((11,)),
            dma((N_SENT,)),
            dma((N_RECEIVED,)),
        ],
        compiler_params=pltpu.CompilerParams(
            collective_id=0, has_side_effects=True, vmem_limit_bytes=VMEM_GRANT
        ),
    )(*(pltpu.with_memory_space_constraint(a, pltpu.HBM) for a in args))
    matrix = jax.ShapeDtypeStruct((ROWS, HD), F32)
    whole = jax.ShapeDtypeStruct((D, HD), BF)
    moment = jax.ShapeDtypeStruct((LOW, HD), F32)
    return pl.pallas_call(
        finish,
        name="finish",
        out_shape=(matrix, matrix, whole, moment, moment) * 2,
        in_specs=[vmem] * 5,
        out_specs=(hbm,) * 10,
        scratch_shapes=[
            pltpu.VMEM((2, FN, ROWS, HD), F32),
            pltpu.VMEM((2, ROWS, HD), F32),
            pltpu.VMEM((2, ROWS, HD), F32),
            pltpu.VMEM((2, D, HD), BF),
            dma((8 + 2 * GROUPS,)),
        ],
        compiler_params=pltpu.CompilerParams(vmem_limit_bytes=VMEM_GRANT),
    )(*handed)


def solution(mesh):
    torus = Mesh(mesh.devices.reshape(YN, XN, ZN, CN), AXES)
    split = P(FS, TP)
    in_specs = (split,) * 5 + (P(FS, None),) * 2 + (split,) * 4
    out_specs = (split, split, P(None, TP), split, split) * 2
    return jax.shard_map(body, mesh=torus, in_specs=in_specs, out_specs=out_specs, check_vma=False)
```
